128 devices in a mesh: ep: 32 (over z, y, core), tp: 4 (over x).
Axes of the slice: x: 4, y: 4, z: 4, core: 2. Of those that a mesh axis runs over, the one named last changes fastest.
Arguments:
- query_rows: bfloat16 [65536, 1024], P('ep', 'tp'), may hold values from -6 to 6
- key_rows: bfloat16 [65536, 1024], P('ep', 'tp'), may hold values from -6 to 6
- value_rows: bfloat16 [65536, 2048], P('ep', 'tp'), may hold values from -6 to 6
- gate_rows: bfloat16 [65536, 2048], P('ep', 'tp'), may hold values from -6 to 6
- log_decay: float32 [8, 65536], P('tp', 'ep'), may hold values from -1 to 0
- out_proj: bfloat16 [2048, 2048], P('tp'), may hold values from -0.125 to 0.125
- moe_input: bfloat16 [16384, 2048], P(('ep', 'tp')), may hold values from -6 to 6
- norm_gain: float32 [2048], replicated, may hold values from 0.1 to 1.9
- routing: int32 [16384, 4], P(('ep', 'tp')), may hold values from 0 to 127, all different within a row; in each aligned block of 128 rows (0 to 127, 128 to 255, ...) at most 8 rows name the same one
- route_weight: float32 [16384, 4], P(('ep', 'tp')), may hold values from 0.2 to 1
- expert_gate: bfloat16 [128, 2048, 512], P(('ep', 'tp')), may hold values from -0.125 to 0.125
- expert_up: bfloat16 [128, 2048, 512], P(('ep', 'tp')), may hold values from -0.125 to 0.125
- expert_down: bfloat16 [128, 512, 2048], P(('ep', 'tp')), may hold values from -0.25 to 0.25
- shared_gate: bfloat16 [2048, 512], replicated, may hold values from -0.125 to 0.125
- shared_up: bfloat16 [2048, 512], replicated, may hold values from -0.125 to 0.125
- shared_down: bfloat16 [512, 2048], replicated, may hold values from -0.25 to 0.25
Outputs:
- mixer_out: bfloat16 [65536, 2048], P(('ep', 'tp'))
- moe_out: bfloat16 [16384, 2048], P(('ep', 'tp'))
The draws below stay inside these ranges and needn't reach their ends.
Inputs may be any that keep to these rules, and one draw needn't show every extreme that they name: `routing`: within the rows of one device no expert is named more than 8 times.
All inputs are finite; a program needn't handle non-finite values.
Results may differ from the reference program's by a relative error of at most 0.019.
Values may be sent and summed in bfloat16 or wider, within the bound.
A program may use at most 128 MiB of HBM per device.

```python
import math
import jax
import jax.numpy as jnp
import numpy as np
from jax import lax

D = 2048
RETENTION_HEADS = 8
DK = 128
DV = 256
BLOCK = 128
TOK_A = 2048
TOKENS_A = 65536
FF = 512
SHARED_FF = 512
TOP = 4
TOK_B = 128
TOKENS_B = 16384
EXPERTS = 128
CAP = 8
N_EP = 32
N_TP = 4


def draw_log_decay(key, part):
    random_subkeys = jax.random.split(jax.random.fold_in(key, 17), 7)
    sequence_length = TOKENS_A
    fast_share = 0.5
    quick_decay_mask = jax.random.uniform(random_subkeys[0], (RETENTION_HEADS,)) < fast_share
    fast_rate = jnp.log(10.0) / jax.random.uniform(random_subkeys[1], (RETENTION_HEADS,), minval=30.0, maxval=100.0)
    slow_rate = jax.random.uniform(random_subkeys[2], (RETENTION_HEADS,), minval=0.2, maxval=0.6) / sequence_length
    base_rate = jnp.where(quick_decay_mask, fast_rate, slow_rate)
    position_index = jnp.arange(sequence_length)
    span_factor = jnp.exp(jax.random.uniform(random_subkeys[3], (sequence_length // TOK_A,), minval=-0.7, maxval=0.7))
    jitter = jnp.exp(jax.random.uniform(random_subkeys[4], (RETENTION_HEADS, sequence_length), minval=-0.35, maxval=0.35))
    chosen_places = jax.random.randint(random_subkeys[5], (3,), 0, sequence_length)
    spike_selected = jnp.any(position_index[None, :] == chosen_places[:, None], axis=0)
    spike_dropped = jnp.log(jax.random.uniform(random_subkeys[6], (RETENTION_HEADS, sequence_length), minval=0.5, maxval=0.8))
    smoothed_decay = -base_rate[:, None] * span_factor[position_index // TOK_A][None, :] * jitter
    selected_mask = spike_selected[None, :] & jnp.logical_not(quick_decay_mask)[:, None]
    return jnp.where(selected_mask, smoothed_decay + spike_dropped, smoothed_decay).astype(jnp.float32)


def steps_of(rng, shape, cuts, smallest, top_value):
    def one(dim, shards_of):
        steps = jax.random.uniform(jax.random.fold_in(jax.random.fold_in(rng, 6), dim), (shards_of,), jnp.float32, smallest / len(cuts), top_value / len(cuts))
        return jnp.repeat(jnp.exp(steps), shape[dim] // shards_of).reshape((-1,) + (1,) * (len(shape) - dim - 1))

    loudness = one(*cuts[0])
    for cut in cuts[1:]:
        loudness = loudness * one(*cut)
    return loudness


def deal_out(rng, own, number, rows, count, top, limit, skew):
    sequence = jax.random.permutation(rng, count)
    crowded, common = portions_of(count, rows * top, limit, skew, True), portions_of(count, rows * top, limit, skew, False)
    places = jnp.arange(count)

    def named(tallies, rotation):
        used = int((tallies > 0).sum())
        fixed = max(1, used // 4)
        passed = fixed + (places - fixed + rotation * (used - fixed)) % max(1, count - fixed)
        return jnp.zeros((count,), jnp.int32).at[sequence[jnp.where(places < fixed, places, passed)]].set(jnp.asarray(tallies, jnp.int32))

    tallies = jnp.where(number % 4 == 0, named(crowded, number // 4), named(common, number - number // 4 - 1))
    mixed = jax.random.permutation(jax.random.fold_in(own, 3), count)
    giver, taker = mixed[0:count // 2 * 2:2], mixed[1:count // 2 * 2:2]
    margin = jnp.minimum(tallies[giver] - 1, limit - tallies[taker]) // 2
    margin = jnp.where((giver == sequence[0]) | (taker == sequence[0]) | (tallies[taker] == 0), 0, jnp.maximum(margin, 0))
    passed = jax.random.randint(jax.random.fold_in(own, 4), (count // 2,), 0, 1 << 20) % (margin + 1)
    tallies = tallies.at[giver].add(-passed).at[taker].add(passed)
    items = jnp.searchsorted(jnp.cumsum(tallies), jnp.arange(rows * top), side="right").astype(jnp.int32)
    listing = items.reshape(top, rows).T
    listing = listing[jax.random.permutation(jax.random.fold_in(own, 1), rows)]
    rotation = jax.random.randint(jax.random.fold_in(own, 2), (rows, 1), 0, top)
    return jnp.take_along_axis(listing, (jnp.arange(top)[None, :] + rotation) % top, axis=1)


def portions_of(number_of, total, most, skew, full):
    portions = [(1 << 20) // math.isqrt(rank ** skew) + 1 for rank in range(1, number_of + 1)]
    largest = most if full else min(most, max(-(-total // number_of), total * portions[0] // sum(portions)))
    least = 1 if total - largest >= number_of - 1 else 0
    given, spare = [largest] + [least] * (number_of - 1), total - largest - least * (number_of - 1)
    while spare > 0:
        candidates = [i for i in range(1, number_of) if given[i] < largest] or [i for i in range(1, number_of) if given[i] < most]
        whole, budget = sum([portions[i] for i in candidates]), spare
        for i in candidates:
            more = min(most - given[i], max(1, budget * portions[i] // whole), spare)
            given[i] = given[i] + more
            spare = spare - more
    return np.array(given)


def bell_draw(rng, shape, width, reach, pieces=(), held_as=jnp.bfloat16):
    loudness = steps_of(rng, shape, pieces, -0.22, 0.18) if pieces else 1.0
    entries = jax.random.normal(rng, shape, jnp.float32) * width * loudness
    return jnp.minimum(jnp.maximum(entries, -reach), reach).astype(held_as)


def setup_inputs(seed: int = 0) -> dict:
    keys = jax.random.split(jax.random.key(seed), 17)
    query_rows = bell_draw(keys[0], (TOKENS_A, RETENTION_HEADS * DK), 1.0, 6.0, ((0, 32), (1, 4)))
    key_rows = bell_draw(keys[1], (TOKENS_A, RETENTION_HEADS * DK), 1.0, 6.0, ((0, 32), (1, 4)))
    value_rows = bell_draw(keys[2], (TOKENS_A, RETENTION_HEADS * DV), 1.0, 6.0, ((0, 32), (1, 4)))
    gate_rows = bell_draw(keys[3], (TOKENS_A, RETENTION_HEADS * DV), 1.0, 6.0, ((0, 32), (1, 4)))
    log_decay = draw_log_decay(jax.random.fold_in(keys[16], 71), 0)
    out_proj = bell_draw(keys[5], (RETENTION_HEADS * DV, D), (RETENTION_HEADS * DV) ** -0.5, 0.125, ((0, 4),))
    moe_input = bell_draw(keys[6], (TOKENS_B, D), 1.0, 6.0, ((0, 128),))
    norm_gain = jnp.clip(1.0 + 0.18 * jax.random.normal(keys[7], (D,), jnp.float32), 0.1, 1.9)
    routing_keys = jax.random.split(jax.random.fold_in(keys[8], 1), TOKENS_B // TOK_B)
    routing_turns = jax.random.permutation(jax.random.fold_in(keys[8], 3), TOKENS_B // TOK_B)
    routing = jax.vmap(lambda own, number: deal_out(jax.random.fold_in(keys[8], 2), own, number, TOK_B, EXPERTS, TOP, CAP, 2))(routing_keys, routing_turns).reshape((TOKENS_B, TOP))
    route_weight = jnp.clip(0.2 + 0.8 * jax.random.uniform(keys[9], (TOKENS_B, TOP), jnp.float32) ** steps_of(keys[9], (TOKENS_B, TOP), ((0, 128),), -0.2, 0.2), 0.2, 1.0)
    expert_gate = bell_draw(keys[10], (EXPERTS, D, FF), D ** -0.5, 0.125, ((0, 128),))
    expert_up = bell_draw(keys[11], (EXPERTS, D, FF), D ** -0.5, 0.125, ((0, 128),))
    expert_down = bell_draw(keys[12], (EXPERTS, FF, D), FF ** -0.5, 0.25, ((0, 128),))
    shared_gate = bell_draw(keys[13], (D, SHARED_FF), D ** -0.5, 0.125)
    shared_up = bell_draw(keys[14], (D, SHARED_FF), D ** -0.5, 0.125)
    shared_down = bell_draw(keys[15], (SHARED_FF, D), SHARED_FF ** -0.5, 0.25)
    return {"query_rows": query_rows, "key_rows": key_rows, "value_rows": value_rows, "gate_rows": gate_rows, "log_decay": log_decay, "out_proj": out_proj, "moe_input": moe_input, "norm_gain": norm_gain, "routing": routing, "route_weight": route_weight, "expert_gate": expert_gate, "expert_up": expert_up, "expert_down": expert_down, "shared_gate": shared_gate, "shared_up": shared_up, "shared_down": shared_down}


EPS = 1e-06

def retention_all(query_rows, key_rows, value_rows, log_decay):
    n_blocks = TOKENS_A // BLOCK
    score_scale = DK ** (-0.5)
    q_blocks = query_rows.reshape(n_blocks, BLOCK, RETENTION_HEADS, DK)
    k_blocks = key_rows.reshape(n_blocks, BLOCK, RETENTION_HEADS, DK)
    v_blocks = value_rows.reshape(n_blocks, BLOCK, RETENTION_HEADS, DV)
    a_blocks = jnp.transpose(log_decay.reshape(RETENTION_HEADS, n_blocks, BLOCK), (1, 0, 2))
    causal = jnp.arange(BLOCK)[:, None] >= jnp.arange(BLOCK)[None, :]

    def advance(carried_state, block_in):
        q_blk, k_blk, v_blk, a_blk = block_in
        cum_decay = jnp.cumsum(a_blk, axis=1)
        block_count = cum_decay[:, -1]
        query_float = q_blk.astype(jnp.float32)
        key_float = k_blk.astype(jnp.float32)
        value_float = v_blk.astype(jnp.float32)
        retention_scores = jnp.einsum('gab,lab->agl', query_float, key_float)
        log_gap = jnp.where(causal[None], cum_decay[:, :, None] - cum_decay[:, None, :], 0.0)
        decay_mat = jnp.where(causal[None], jnp.exp(log_gap), 0.0)
        weight = (retention_scores * score_scale * decay_mat).astype(jnp.bfloat16)
        weight = lax.optimization_barrier(weight).astype(jnp.float32)
        inner_out = jnp.einsum('hnm,mhe->nhe', weight, value_float)
        state_low = lax.optimization_barrier(carried_state.astype(jnp.bfloat16)).astype(jnp.float32)
        cross_out = jnp.einsum('nhd,hde->nhe', query_float, state_low) * jnp.exp(cum_decay).T[:, :, None]
        decayed_key_rows = (key_float * score_scale * jnp.exp(block_count[None, :] - cum_decay.T)[:, :, None]).astype(jnp.bfloat16)
        decayed_key_rows = lax.optimization_barrier(decayed_key_rows).astype(jnp.float32)
        carried_state = carried_state * jnp.exp(block_count)[:, None, None] + jnp.einsum('czq,czy->zqy', decayed_key_rows, value_float)
        return (carried_state, inner_out + cross_out)
    initial = jnp.zeros((RETENTION_HEADS, DK, DV), jnp.float32)
    _, outputs = lax.scan(advance, initial, (q_blocks, k_blocks, v_blocks, a_blocks))
    return outputs.reshape(TOKENS_A, RETENTION_HEADS, DV)

def expert_apply(inputs, w_gate, w_up, w_down):
    gate_act = jnp.dot(inputs, w_gate, preferred_element_type=jnp.float32)
    up_act = jnp.dot(inputs, w_up, preferred_element_type=jnp.float32)
    hidden = (jax.nn.silu(gate_act) * up_act).astype(jnp.bfloat16)
    return jnp.dot(hidden, w_down, preferred_element_type=jnp.float32)

def reference(query_rows, key_rows, value_rows, gate_rows, log_decay, out_proj, moe_input, norm_gain, routing, route_weight, expert_gate, expert_up, expert_down, shared_gate, shared_up, shared_down):
    raw_out = retention_all(query_rows, key_rows, value_rows, log_decay)
    avg_out = lax.optimization_barrier(jnp.mean(raw_out, axis=-1, keepdims=True))
    spread = lax.optimization_barrier(jnp.mean(jnp.square(raw_out - avg_out), axis=-1, keepdims=True))
    normed = (raw_out - avg_out) * lax.rsqrt(spread + EPS)
    gate_act = jax.nn.silu(gate_rows.astype(jnp.float32).reshape(TOKENS_A, RETENTION_HEADS, DV))
    retained = (gate_act * normed).reshape(TOKENS_A, RETENTION_HEADS * DV).astype(jnp.bfloat16)
    group_cols = RETENTION_HEADS * DV // N_TP
    summed = jnp.zeros((TOKENS_A, D), jnp.float32)
    for group_idx in range(N_TP):
        lo_col = group_idx * group_cols
        partial_sum = jnp.dot(retained[:, lo_col:lo_col + group_cols], out_proj[lo_col:lo_col + group_cols], preferred_element_type=jnp.float32).astype(jnp.bfloat16)
        summed = summed + partial_sum.astype(jnp.float32)
    mixer_out = summed.astype(jnp.bfloat16)
    as_float = moe_input.astype(jnp.float32)
    moe_normed = (as_float * lax.rsqrt(lax.optimization_barrier(jnp.mean(as_float * as_float, axis=-1, keepdims=True)) + EPS) * norm_gain).astype(jnp.bfloat16)
    flat_route = routing.reshape(-1)
    flat_weight = route_weight.reshape(-1)
    bound_rows = N_EP * N_TP * CAP

    def visit(total_out, expert_idx):
        picked_rows = jnp.nonzero(flat_route == expert_idx, size=bound_rows, fill_value=0)[0].astype(jnp.int32)
        live_mask = (jnp.arange(bound_rows) < jnp.sum((flat_route == expert_idx).astype(jnp.int32))).astype(jnp.float32)
        token_idx = picked_rows // TOP
        result = expert_apply(moe_normed[token_idx], expert_gate[expert_idx], expert_up[expert_idx], expert_down[expert_idx])
        result = lax.optimization_barrier(result.astype(jnp.bfloat16)).astype(jnp.float32)
        scaled = result * (flat_weight[picked_rows] * live_mask)[:, None]
        return (total_out.at[token_idx].add(scaled), None)
    routed, _ = lax.scan(visit, jnp.zeros((TOKENS_B, D), jnp.float32), jnp.arange(N_EP * N_TP, dtype=jnp.int32))
    shared = expert_apply(moe_normed, shared_gate, shared_up, shared_down)
    moe_out = (routed + shared).astype(jnp.bfloat16)
    return (mixer_out, moe_out)
```

```python
import functools

import jax
import jax.numpy as jnp
from jax import lax
from jax.experimental import pallas as pl
from jax.experimental.pallas import tpu as pltpu
from jax.sharding import Mesh
from jax.sharding import PartitionSpec as P

DK = 128
DV = 256
BLOCK = 128
EP = ("ep_0", "ep_1", "ep_2")
EP_TP = ("ep_0", "ep_1", "ep_2", "tp")
EPS = 1e-06
MESH = pl.DeviceIdType.MESH
HI = lax.Precision.HIGHEST
F32 = jnp.float32
BF16 = jnp.bfloat16
SCALE = DK ** (-0.5)

NT = (((1,), (1,)), ((), ()))
TN = (((0,), (0,)), ((), ()))


def dot(a, b, dims=None, precision=None):
    if dims is None:
        dims = (((1,), (0,)), ((), ()))
    return lax.dot_general(a, b, dims, precision=precision, preferred_element_type=F32)


def iota(shape, dim):
    return lax.broadcasted_iota(jnp.int32, shape, dim)


def silu(v):
    half = 0.5 * v
    return half * jnp.tanh(half) + half


N_BLK = 16
HEADS = 2
PAY = DK + 16


def mixer_kernel(
    q_ref, k_ref, v_ref, g_ref, ld_ref, wo_ref, out_ref,
    W, R, ret, inner, prev, a_s, c_s, e_s, run, inc, tot_S, tot_f, bef_S, bef_f,
    pay, got_c, got_y, got_z,
    wx_s, wx_r, w1_s, w1_r, w2_s, w2_r, w3_s, w3_r, pre_s, pre_r, ret_s, ret_r, loc_sem,
):
    z = lax.axis_index("ep_0")
    y = lax.axis_index("ep_1")
    c = lax.axis_index("ep_2")
    x = lax.axis_index("tp")
    place = {"ep_0": z, "ep_1": y, "ep_2": c, "tp": x}
    size = {"ep_0": 4, "ep_1": 4, "ep_2": 2, "tp": 4}

    def peer(axis, d):
        return {axis: lax.rem(place[axis] + d, size[axis])}

    links = [(a, d) for a in ("ep_0", "ep_1", "tp") for d in (1, 2, 3)] + [("ep_2", 1)]
    barrier = pltpu.get_barrier_semaphore()
    for a, d in links:
        pl.semaphore_signal(barrier, inc=1, device_id=peer(a, d), device_id_type=MESH)
    pl.semaphore_wait(barrier, len(links))

    def rows(start, n):
        return pl.ds(pl.multiple_of(start, 16), n)

    half0, half1 = pl.ds(0, 1024), pl.ds(1024, 1024)
    r0 = c * 256 + y * 64 + z * 16
    r1 = c * 256 + z * 64 + y * 16

    own_w = pltpu.make_async_copy(wo_ref, W.at[0], loc_sem)
    own_w.start()
    wx = []
    for d in (1, 2, 3):
        for h, (r, cols) in enumerate(((r0, half0), (r1, half1))):
            i = (d - 1) * 2 + h
            cp = pltpu.make_async_remote_copy(
                src_ref=wo_ref.at[rows(r, 16), cols],
                dst_ref=W.at[4 - d, rows(r, 16), cols],
                send_sem=wx_s.at[i],
                recv_sem=wx_r.at[i],
                device_id=peer("tp", d),
                device_id_type=MESH,
            )
            cp.start()
            wx.append(cp)

    for h in range(HEADS):
        for j in range(N_BLK):
            a_s[h * N_BLK + j : h * N_BLK + j + 1, :] = ld_ref[h : h + 1, j * BLOCK : (j + 1) * BLOCK]
    a = a_s[...]
    upper = (iota((BLOCK, BLOCK), 0) <= iota((BLOCK, BLOCK), 1)).astype(F32)
    cum = dot(a, upper, precision=HI)
    c_s[...] = cum
    nb = HEADS * N_BLK
    totb = jnp.broadcast_to(cum[:, BLOCK - 1 : BLOCK], (nb, BLOCK))
    ri, ci = iota((nb, nb), 0), iota((nb, nb), 1)
    same = (ri // N_BLK) == (ci // N_BLK)
    after = dot((same & (ci > ri)).astype(F32), totb, precision=HI)
    e_s[...] = jnp.exp(after + totb - cum) * SCALE
    whole = jnp.exp(after + totb)

    run[...] = jnp.zeros_like(run)

    def col(row):
        return jnp.broadcast_to(row, (BLOCK, BLOCK)).T

    def summary(j, _):
        sl = pl.ds(pl.multiple_of(j * BLOCK, BLOCK), BLOCK)
        for h in range(HEADS):
            kb = k_ref[sl, h * DK : (h + 1) * DK].astype(F32)
            vb = v_ref[sl, h * DV : (h + 1) * DV]
            kd = (kb * col(e_s[pl.ds(h * N_BLK + j, 1), :])).astype(BF16)
            run[h] += dot(kd, vb, TN)
        return 0

    lax.fori_loop(0, N_BLK, summary, 0)
    for h in range(HEADS):
        f = whole[h * N_BLK : h * N_BLK + 1, :]
        tot_f[h] = jnp.concatenate([f, f], axis=1)
        tot_S[h] = run[h]
        bef_S[h] = jnp.zeros((DK, DV), F32)
        bef_f[h] = jnp.ones((1, DV), F32)

    def publish(axis, got, base):
        for h in range(HEADS):
            pay[h, 0:DK, :] = tot_S[h].astype(BF16)
            f = tot_f[h]
            f1 = f.astype(BF16)
            f2 = (f - f1.astype(F32)).astype(BF16)
            row = iota((16, DV), 0)
            top = jnp.where(row == 0, f1.astype(F32), jnp.where(row == 1, f2.astype(F32), 0.0))
            pay[h, DK:PAY, :] = top.astype(BF16)
        cps = []
        for d in range(1, size[axis]):
            cp = pltpu.make_async_remote_copy(
                src_ref=pay,
                dst_ref=got.at[d - 1],
                send_sem=pre_s.at[base + d - 1],
                recv_sem=pre_r.at[base + d - 1],
                device_id=peer(axis, d),
                device_id_type=MESH,
            )
            cp.start()
            cps.append(cp)
        return cps

    def absorb(axis, got, cps):
        n, at = size[axis], place[axis]
        for cp in cps:
            cp.wait()
        for h in range(HEADS):
            sub_f = jnp.ones((1, DV), F32)
            sub_S = jnp.zeros((DK, DV), F32)
            in_f, in_S = sub_f, sub_S
            for k in range(n):
                own = at == k
                slot = jnp.maximum(lax.rem(at - k + n, n) - 1, 0)
                piece = got[slot, h].astype(F32)
                pf = piece[DK : DK + 1, :] + piece[DK + 1 : DK + 2, :]
                pf = jnp.where(own, tot_f[h], pf)
                ps = jnp.where(own, tot_S[h], piece[0:DK, :])
                if k:
                    in_f = jnp.where(own, sub_f, in_f)
                    in_S = jnp.where(own, sub_S, in_S)
                sub_S = pf * sub_S + ps
                sub_f = sub_f * pf
            bef_S[h] = bef_f[h] * in_S + bef_S[h]
            bef_f[h] = bef_f[h] * in_f
            tot_S[h] = sub_S
            tot_f[h] = sub_f

    causal = iota((BLOCK, BLOCK), 0) >= iota((BLOCK, BLOCK), 1)
    run[...] = jnp.zeros_like(run)

    def inside(j, _):
        sl = pl.ds(pl.multiple_of(j * BLOCK, BLOCK), BLOCK)
        for h in range(HEADS):
            qb = q_ref[sl, h * DK : (h + 1) * DK]
            kb = k_ref[sl, h * DK : (h + 1) * DK]
            vb = v_ref[sl, h * DV : (h + 1) * DV]
            crow = c_s[pl.ds(h * N_BLK + j, 1), :]
            ccol = col(crow)
            gap = ccol - jnp.broadcast_to(crow, (BLOCK, BLOCK))
            dec = jnp.exp(jnp.where(causal, gap, -1e30)) * SCALE
            w = (dot(qb, kb, NT) * dec).astype(BF16)
            inner[sl, h * DV : (h + 1) * DV] = dot(w, vb)
            last = crow[:, BLOCK - 1 : BLOCK]
            kd = (kb.astype(F32) * (jnp.exp(last - ccol) * SCALE)).astype(BF16)
            prev[h * N_BLK + j] = run[h]
            run[h] = run[h] * jnp.exp(last) + dot(kd, vb, TN)
        return 0

    cps = publish("ep_2", got_c, 0)
    lax.fori_loop(0, 5, inside, 0)
    absorb("ep_2", got_c, cps)
    cps = publish("ep_1", got_y, 1)
    lax.fori_loop(5, 10, inside, 0)

    for cp in wx:
        cp.wait()

    def spread(axis, d, r, n, cols, ss, rs):
        return pltpu.make_async_remote_copy(
            src_ref=W.at[1:4, rows(r, n), cols],
            dst_ref=W.at[1:4, rows(r, n), cols],
            send_sem=ss,
            recv_sem=rs,
            device_id=peer(axis, d),
            device_id_type=MESH,
        )

    first, first_in = [], []
    for d in (1, 2, 3):
        zf = lax.rem(z + 4 - d, 4)
        yf = lax.rem(y + 4 - d, 4)
        for h, (axis, r, rf, cols) in enumerate(
            (
                ("ep_0", r0, c * 256 + y * 64 + zf * 16, half0),
                ("ep_1", r1, c * 256 + z * 64 + yf * 16, half1),
            )
        ):
            i = (d - 1) * 2 + h
            cp = spread(axis, d, r, 16, cols, w1_s.at[i], w1_r.at[i])
            cp.start()
            first.append(cp)
            first_in.append(spread(axis, d, rf, 16, cols, w1_s.at[i], w1_r.at[i]))

    absorb("ep_1", got_y, cps)
    cps = publish("ep_0", got_z, 4)
    lax.fori_loop(10, N_BLK, inside, 0)
    for cp in first_in:
        cp.wait_recv()

    second, second_in = [], []
    for d in (1, 2, 3):
        zf = lax.rem(z + 4 - d, 4)
        yf = lax.rem(y + 4 - d, 4)
        for h, (axis, r, rf, cols) in enumerate(
            (
                ("ep_1", c * 256 + y * 64, c * 256 + yf * 64, half0),
                ("ep_0", c * 256 + z * 64, c * 256 + zf * 64, half1),
            )
        ):
            i = (d - 1) * 2 + h
            cp = spread(axis, d, r, 64, cols, w2_s.at[i], w2_r.at[i])
            cp.start()
            second.append(cp)
            second_in.append(spread(axis, d, rf, 64, cols, w2_s.at[i], w2_r.at[i]))

    absorb("ep_0", got_z, cps)
    for h in range(HEADS):
        inc[h] = bef_S[h]

    def outer(j, _):
        sl = pl.ds(pl.multiple_of(j * BLOCK, BLOCK), BLOCK)
        for h in range(HEADS):
            qb = q_ref[sl, h * DK : (h + 1) * DK]
            crow = c_s[pl.ds(h * N_BLK + j, 1), :]
            grow = jnp.exp(col(crow))
            grow = jnp.concatenate([grow, grow], axis=1)
            state = inc[h]
            cross = dot(qb, (prev[h * N_BLK + j] + state).astype(BF16))
            inc[h] = state * jnp.exp(crow[:, BLOCK - 1 : BLOCK])
            raw = inner[sl, h * DV : (h + 1) * DV] + cross * grow
            d = raw - jnp.mean(raw, axis=-1, keepdims=True)
            n = d * lax.rsqrt(jnp.mean(d * d, axis=-1, keepdims=True) + EPS)
            gate = silu(g_ref[sl, h * DV : (h + 1) * DV].astype(F32))
            ret[sl, h * DV : (h + 1) * DV] = (gate * n).astype(BF16)
        return 0

    sends = []
    for d in (1, 2, 3, 0):
        p = lax.rem(x + d, 4)
        lax.fori_loop(p * 4, p * 4 + 4, outer, 0) if False else None
    lax.fori_loop(0, N_BLK, outer, 0)
    for d in (1, 2, 3):
        p = lax.rem(x + d, 4)
        cp = pltpu.make_async_remote_copy(
            src_ref=ret.at[rows(p * 512, 512), :],
            dst_ref=R.at[3 - d],
            send_sem=ret_s.at[d - 1],
            recv_sem=ret_r.at[d - 1],
            device_id=peer("tp", d),
            device_id_type=MESH,
        )
        cp.start()
        sends.append(cp)

    for cp in second_in:
        cp.wait_recv()
    own_half = c * 256
    other_half = (1 - c) * 256
    third = spread("ep_2", 1, own_half, 256, pl.ds(0, 2048), w3_s, w3_r)
    third.start()
    third_in = spread("ep_2", 1, other_half, 256, pl.ds(0, 2048), w3_s, w3_r)
    own_w.wait()
    for cp in sends:
        cp.wait_recv()
    third_in.wait_recv()

    def project(t, _):
        cols = pl.ds(pl.multiple_of(t * 512, 512), 512)
        acc = dot(ret[rows(x * 512, 512), :], W[0, :, cols])
        for g in (1, 2, 3):
            acc += dot(R[g - 1], W[g, :, cols])
        out_ref[:, cols] = acc.astype(BF16)
        return 0

    lax.fori_loop(0, 4, project, 0)
    for cp in first + second + sends + [third]:
        cp.wait_send()


def mixer_half(q, k, v, g, ld, wo):
    vm = pl.BlockSpec(memory_space=pltpu.VMEM)
    dma = pltpu.SemaphoreType.DMA
    return pl.pallas_call(
        mixer_kernel,
        name="mixer",
        out_shape=jax.ShapeDtypeStruct((512, 2048), BF16),
        in_specs=[vm, vm, vm, vm, vm, pl.BlockSpec(memory_space=pl.ANY)],
        out_specs=vm,
        scratch_shapes=[
            pltpu.VMEM((4, 512, 2048), BF16),
            pltpu.VMEM((3, 512, 512), BF16),
            pltpu.VMEM((2048, 512), BF16),
            pltpu.VMEM((2048, 512), F32),
            pltpu.VMEM((32, DK, DV), F32),
            pltpu.VMEM((32, BLOCK), F32),
            pltpu.VMEM((32, BLOCK), F32),
            pltpu.VMEM((32, BLOCK), F32),
            pltpu.VMEM((2, DK, DV), F32),
            pltpu.VMEM((2, DK, DV), F32),
            pltpu.VMEM((2, DK, DV), F32),
            pltpu.VMEM((2, 1, DV), F32),
            pltpu.VMEM((2, DK, DV), F32),
            pltpu.VMEM((2, 1, DV), F32),
            pltpu.VMEM((2, PAY, DV), BF16),
            pltpu.VMEM((1, 2, PAY, DV), BF16),
            pltpu.VMEM((3, 2, PAY, DV), BF16),
            pltpu.VMEM((3, 2, PAY, DV), BF16),
            dma((6,)), dma((6,)), dma((6,)), dma((6,)), dma((6,)), dma((6,)), dma, dma,
            dma((7,)), dma((7,)), dma((3,)), dma((3,)), dma,
        ],
        compiler_params=pltpu.CompilerParams(
            collective_id=0, has_side_effects=True, vmem_limit_bytes=50 * 1024 * 1024
        ),
        cost_estimate=pl.CostEstimate(flops=40_000_000_000, bytes_accessed=16_000_000, transcendentals=2_000_000),
    )(q, k, v, g, ld, wo)


SLOTS = 1024
CAP = 8
N_TOK = 128
N_EXP = 128
TOP = 4


def slot_matrix(routing, values=None):
    lane = iota((N_TOK, N_EXP), 1)
    named = jnp.zeros((N_TOK, N_EXP), F32)
    for kk in range(TOP):
        named = named + (routing[:, kk : kk + 1] == lane).astype(F32)
    named = named.astype(BF16)
    lower = (iota((N_TOK, N_TOK), 0) > iota((N_TOK, N_TOK), 1)).astype(BF16)
    rank = dot(lower, named).astype(BF16)
    slot = iota((SLOTS, N_EXP), 0)
    spread = (slot // CAP == iota((SLOTS, N_EXP), 1)).astype(BF16)
    at = (slot % CAP).astype(F32)
    live = (dot(spread, named, NT) > 0.5) & (dot(spread, rank, NT) == at)
    if values is None:
        return live.astype(BF16)
    weight = jnp.zeros((N_TOK, N_EXP), F32)
    for kk in range(TOP):
        weight = weight + jnp.where(routing[:, kk : kk + 1] == lane, values[:, kk : kk + 1], 0.0)
    hi = weight.astype(BF16)
    lo = (weight - hi.astype(F32)).astype(BF16)
    parts = []
    for part in (hi, lo):
        parts.append(jnp.where(live, dot(spread, part, NT), 0.0).astype(BF16))
    return parts


def normed_rows(x_ref, gain_ref):
    v = x_ref[...].astype(F32)
    return (v * lax.rsqrt(jnp.mean(v * v, axis=-1, keepdims=True) + EPS) * gain_ref[...]).astype(BF16)


def dispatch_kernel(x_ref, gain_ref, routing_ref, out_ref, normed_ref):
    normed_ref[...] = normed_rows(x_ref, gain_ref)
    place = slot_matrix(routing_ref[...])
    for t in range(4):
        cols = slice(t * 512, (t + 1) * 512)
        out_ref[:, cols] = dot(place, normed_ref[:, cols]).astype(BF16)


def dispatch(x, gain, routing):
    vm = pl.BlockSpec(memory_space=pltpu.VMEM)
    return pl.pallas_call(
        dispatch_kernel,
        name="dispatch",
        out_shape=(jax.ShapeDtypeStruct((SLOTS, 2048), BF16), jax.ShapeDtypeStruct((N_TOK, 2048), BF16)),
        in_specs=[vm] * 3,
        out_specs=(vm, vm),
        compiler_params=pltpu.CompilerParams(vmem_limit_bytes=32 * 1024 * 1024),
    )(x, gain, routing)


def expert_kernel(rows_ref, wg_ref, wu_ref, wd_ref, out_ref):
    rows = rows_ref[...]
    hidden = (silu(dot(rows, wg_ref[...])) * dot(rows, wu_ref[...])).astype(BF16)
    out_ref[...] = dot(hidden, wd_ref[...]).astype(out_ref.dtype)


def expert(rows, wg, wu, wd, dtype, step):
    n = rows.shape[0]
    whole = lambda w: pl.BlockSpec(w.shape, lambda i: (0, 0))
    return pl.pallas_call(
        expert_kernel,
        name="expert",
        grid=(n // step,),
        out_shape=jax.ShapeDtypeStruct((n, 2048), dtype),
        in_specs=[pl.BlockSpec((step, 2048), lambda i: (i, 0)), whole(wg), whole(wu), whole(wd)],
        out_specs=pl.BlockSpec((step, 2048), lambda i: (i, 0)),
        compiler_params=pltpu.CompilerParams(vmem_limit_bytes=40 * 1024 * 1024),
        cost_estimate=pl.CostEstimate(flops=6 * n * 2048 * 512, bytes_accessed=15_000_000, transcendentals=0),
    )(rows, wg, wu, wd)


def combine_kernel(back_ref, routing_ref, weight_ref, shared_ref, out_ref):
    hi, lo = slot_matrix(routing_ref[...], weight_ref[...])
    for t in range(4):
        cols = slice(t * 512, (t + 1) * 512)
        back = back_ref[:, cols]
        total = dot(hi, back, TN) + dot(lo, back, TN) + shared_ref[:, cols]
        out_ref[:, cols] = total.astype(BF16)


def combine(back, routing, weight, shared):
    vm = pl.BlockSpec(memory_space=pltpu.VMEM)
    return pl.pallas_call(
        combine_kernel,
        name="combine",
        out_shape=jax.ShapeDtypeStruct((N_TOK, 2048), BF16),
        in_specs=[vm] * 4,
        out_specs=vm,
        compiler_params=pltpu.CompilerParams(vmem_limit_bytes=32 * 1024 * 1024),
    )(back, routing, weight, shared)


def local(
    query_rows, key_rows, value_rows, gate_rows, log_decay, out_proj,
    moe_input, norm_gain, routing, route_weight,
    expert_gate, expert_up, expert_down, shared_gate, shared_up, shared_down,
):
    slots, normed = dispatch(moe_input, norm_gain.reshape(1, -1), routing)
    exchange = lambda r: lax.all_to_all(
        r.reshape(N_EXP, CAP, 2048), EP_TP, split_axis=0, concat_axis=0, tiled=True
    ).reshape(SLOTS, 2048)
    received = exchange(slots)
    mixer_out = mixer_half(query_rows, key_rows, value_rows, gate_rows, log_decay, out_proj)
    served = expert(received, expert_gate[0], expert_up[0], expert_down[0], BF16, 256)
    returned = exchange(served)
    shared = expert(normed, shared_gate, shared_up, shared_down, F32, 128)
    moe_out = combine(returned, routing, route_weight, shared)
    return (mixer_out, moe_out)


def solution(mesh):
    split = Mesh(mesh.devices.reshape(4, 4, 2, mesh.shape["tp"]), ("ep_0", "ep_1", "ep_2", "tp"))
    return jax.shard_map(
        local,
        mesh=split,
        in_specs=(
            P(EP, "tp"),
            P(EP, "tp"),
            P(EP, "tp"),
            P(EP, "tp"),
            P("tp", EP),
            P("tp", None),
            P(EP_TP, None),
            P(),
            P(EP_TP, None),
            P(EP_TP, None),
            P(EP_TP, None, None),
            P(EP_TP, None, None),
            P(EP_TP, None, None),
            P(),
            P(),
            P(),
        ),
        out_specs=(P(EP_TP, None), P(EP_TP, None)),
        check_vma=False,
    )
```

```python
import functools

import jax
import jax.numpy as jnp
from jax import lax
from jax.experimental import pallas as pl
from jax.experimental.pallas import tpu as pltpu
from jax.sharding import Mesh
from jax.sharding import PartitionSpec as P

DK = 128
DV = 256
BLOCK = 128
EP = ("ep_0", "ep_1", "ep_2")
EP_TP = ("ep_0", "ep_1", "ep_2", "tp")
EPS = 1e-06
MESH = pl.DeviceIdType.MESH
HI = lax.Precision.HIGHEST
F32 = jnp.float32
BF16 = jnp.bfloat16
SCALE = DK ** (-0.5)

NT = (((1,), (1,)), ((), ()))
TN = (((0,), (0,)), ((), ()))


def dot(a, b, dims=None, precision=None):
    if dims is None:
        dims = (((1,), (0,)), ((), ()))
    return lax.dot_general(a, b, dims, precision=precision, preferred_element_type=F32)


def iota(shape, dim):
    return lax.broadcasted_iota(jnp.int32, shape, dim)


def silu(v):
    half = 0.5 * v
    return half * jnp.tanh(half) + half


N_BLK = 16
HEADS = 2
PAY = DK + 16


def mixer_kernel(
    q_ref, k_ref, v_ref, g_ref, ld_ref, wo_ref, out_ref,
    W, R, ret, inner, prev, a_s, c_s, e_s, run, inc, tot_S, tot_f, bef_S, bef_f,
    pay, got_c, got_y, got_z,
    wx_s, wx_r, w1_s, w1_r, w2_s, w2_r, w3_s, w3_r, pre_s, pre_r, ret_s, ret_r, loc_sem,
):
    z = lax.axis_index("ep_0")
    y = lax.axis_index("ep_1")
    c = lax.axis_index("ep_2")
    x = lax.axis_index("tp")
    place = {"ep_0": z, "ep_1": y, "ep_2": c, "tp": x}
    size = {"ep_0": 4, "ep_1": 4, "ep_2": 2, "tp": 4}

    def peer(axis, d):
        return {axis: lax.rem(place[axis] + d, size[axis])}

    links = [(a, d) for a in ("ep_0", "ep_1", "tp") for d in (1, 2, 3)] + [("ep_2", 1)]
    barrier = pltpu.get_barrier_semaphore()
    for a, d in links:
        pl.semaphore_signal(barrier, inc=1, device_id=peer(a, d), device_id_type=MESH)
    pl.semaphore_wait(barrier, len(links))

    def rows(start, n):
        return pl.ds(pl.multiple_of(start, 16), n)

    half0, half1 = pl.ds(0, 1024), pl.ds(1024, 1024)
    r0 = c * 256 + y * 64 + z * 16
    r1 = c * 256 + z * 64 + y * 16

    own_w = pltpu.make_async_copy(wo_ref, W.at[0], loc_sem)
    own_w.start()
    wx = []
    for d in (1, 2, 3):
        for h, (r, cols) in enumerate(((r0, half0), (r1, half1))):
            i = (d - 1) * 2 + h
            cp = pltpu.make_async_remote_copy(
                src_ref=wo_ref.at[rows(r, 16), cols],
                dst_ref=W.at[4 - d, rows(r, 16), cols],
                send_sem=wx_s.at[i],
                recv_sem=wx_r.at[i],
                device_id=peer("tp", d),
                device_id_type=MESH,
            )
            cp.start()
            wx.append(cp)

    for h in range(HEADS):
        for j in range(N_BLK):
            a_s[h * N_BLK + j : h * N_BLK + j + 1, :] = ld_ref[h : h + 1, j * BLOCK : (j + 1) * BLOCK]
    a = a_s[...]
    upper = (iota((BLOCK, BLOCK), 0) <= iota((BLOCK, BLOCK), 1)).astype(F32)
    cum = dot(a, upper, precision=HI)
    c_s[...] = cum
    nb = HEADS * N_BLK
    totb = jnp.broadcast_to(cum[:, BLOCK - 1 : BLOCK], (nb, BLOCK))
    ri, ci = iota((nb, nb), 0), iota((nb, nb), 1)
    same = (ri // N_BLK) == (ci // N_BLK)
    after = dot((same & (ci > ri)).astype(F32), totb, precision=HI)
    e_s[...] = jnp.exp(after + totb - cum) * SCALE
    whole = jnp.exp(after + totb)

    run[...] = jnp.zeros_like(run)

    def col(row):
        return jnp.broadcast_to(row, (BLOCK, BLOCK)).T

    def summary(j, _):
        sl = pl.ds(pl.multiple_of(j * BLOCK, BLOCK), BLOCK)
        for h in range(HEADS):
            kb = k_ref[sl, h * DK : (h + 1) * DK].astype(F32)
            vb = v_ref[sl, h * DV : (h + 1) * DV]
            kd = (kb * col(e_s[pl.ds(h * N_BLK + j, 1), :])).astype(BF16)
            run[h] += dot(kd, vb, TN)
        return 0

    lax.fori_loop(0, N_BLK, summary, 0)
    for h in range(HEADS):
        f = whole[h * N_BLK : h * N_BLK + 1, :]
        tot_f[h] = jnp.concatenate([f, f], axis=1)
        tot_S[h] = run[h]
        bef_S[h] = jnp.zeros((DK, DV), F32)
        bef_f[h] = jnp.ones((1, DV), F32)

    def publish(axis, got, base):
        for h in range(HEADS):
            pay[h, 0:DK, :] = tot_S[h].astype(BF16)
            f = tot_f[h]
            f1 = f.astype(BF16)
            f2 = (f - f1.astype(F32)).astype(BF16)
            row = iota((16, DV), 0)
            top = jnp.where(row == 0, f1.astype(F32), jnp.where(row == 1, f2.astype(F32), 0.0))
            pay[h, DK:PAY, :] = top.astype(BF16)
        cps = []
        for d in range(1, size[axis]):
            cp = pltpu.make_async_remote_copy(
                src_ref=pay,
                dst_ref=got.at[d - 1],
                send_sem=pre_s.at[base + d - 1],
                recv_sem=pre_r.at[base + d - 1],
                device_id=peer(axis, d),
                device_id_type=MESH,
            )
            cp.start()
            cps.append(cp)
        return cps

    def absorb(axis, got, cps):
        n, at = size[axis], place[axis]
        for cp in cps:
            cp.wait()
        for h in range(HEADS):
            sub_f = jnp.ones((1, DV), F32)
            sub_S = jnp.zeros((DK, DV), F32)
            in_f, in_S = sub_f, sub_S
            for k in range(n):
                own = at == k
                slot = jnp.maximum(lax.rem(at - k + n, n) - 1, 0)
                piece = got[slot, h].astype(F32)
                pf = piece[DK : DK + 1, :] + piece[DK + 1 : DK + 2, :]
                pf = jnp.where(own, tot_f[h], pf)
                ps = jnp.where(own, tot_S[h], piece[0:DK, :])
                if k:
                    in_f = jnp.where(own, sub_f, in_f)
                    in_S = jnp.where(own, sub_S, in_S)
                sub_S = pf * sub_S + ps
                sub_f = sub_f * pf
            bef_S[h] = bef_f[h] * in_S + bef_S[h]
            bef_f[h] = bef_f[h] * in_f
            tot_S[h] = sub_S
            tot_f[h] = sub_f

    causal = iota((BLOCK, BLOCK), 0) >= iota((BLOCK, BLOCK), 1)
    run[...] = jnp.zeros_like(run)

    def inside(j, _):
        sl = pl.ds(pl.multiple_of(j * BLOCK, BLOCK), BLOCK)
        for h in range(HEADS):
            qb = q_ref[sl, h * DK : (h + 1) * DK]
            kb = k_ref[sl, h * DK : (h + 1) * DK]
            vb = v_ref[sl, h * DV : (h + 1) * DV]
            crow = c_s[pl.ds(h * N_BLK + j, 1), :]
            ccol = col(crow)
            gap = ccol - jnp.broadcast_to(crow, (BLOCK, BLOCK))
            dec = jnp.exp(jnp.where(causal, gap, -1e30)) * SCALE
            w = (dot(qb, kb, NT) * dec).astype(BF16)
            inner[sl, h * DV : (h + 1) * DV] = dot(w, vb)
            last = crow[:, BLOCK - 1 : BLOCK]
            kd = (kb.astype(F32) * (jnp.exp(last - ccol) * SCALE)).astype(BF16)
            prev[h * N_BLK + j] = run[h]
            run[h] = run[h] * jnp.exp(last) + dot(kd, vb, TN)
        return 0

    cps = publish("ep_2", got_c, 0)
    lax.fori_loop(0, 5, inside, 0)
    absorb("ep_2", got_c, cps)
    cps = publish("ep_1", got_y, 1)
    lax.fori_loop(5, 10, inside, 0)

    for cp in wx:
        cp.wait()

    def spread(axis, d, r, n, cols, ss, rs):
        return pltpu.make_async_remote_copy(
            src_ref=W.at[1:4, rows(r, n), cols],
            dst_ref=W.at[1:4, rows(r, n), cols],
            send_sem=ss,
            recv_sem=rs,
            device_id=peer(axis, d),
            device_id_type=MESH,
        )

    first, first_in = [], []
    for d in (1, 2, 3):
        zf = lax.rem(z + 4 - d, 4)
        yf = lax.rem(y + 4 - d, 4)
        for h, (axis, r, rf, cols) in enumerate(
            (
                ("ep_0", r0, c * 256 + y * 64 + zf * 16, half0),
                ("ep_1", r1, c * 256 + z * 64 + yf * 16, half1),
            )
        ):
            i = (d - 1) * 2 + h
            cp = spread(axis, d, r, 16, cols, w1_s.at[i], w1_r.at[i])
            cp.start()
            first.append(cp)
            first_in.append(spread(axis, d, rf, 16, cols, w1_s.at[i], w1_r.at[i]))

    absorb("ep_1", got_y, cps)
    cps = publish("ep_0", got_z, 4)
    lax.fori_loop(10, N_BLK, inside, 0)
    for cp in first_in:
        cp.wait_recv()

    second, second_in = [], []
    for d in (1, 2, 3):
        zf = lax.rem(z + 4 - d, 4)
        yf = lax.rem(y + 4 - d, 4)
        for h, (axis, r, rf, cols) in enumerate(
            (
                ("ep_1", c * 256 + y * 64, c * 256 + yf * 64, half0),
                ("ep_0", c * 256 + z * 64, c * 256 + zf * 64, half1),
            )
        ):
            i = (d - 1) * 2 + h
            cp = spread(axis, d, r, 64, cols, w2_s.at[i], w2_r.at[i])
            cp.start()
            second.append(cp)
            second_in.append(spread(axis, d, rf, 64, cols, w2_s.at[i], w2_r.at[i]))

    absorb("ep_0", got_z, cps)
    for h in range(HEADS):
        inc[h] = bef_S[h]

    def outer(j, _):
        sl = pl.ds(pl.multiple_of(j * BLOCK, BLOCK), BLOCK)
        for h in range(HEADS):
            qb = q_ref[sl, h * DK : (h + 1) * DK]
            crow = c_s[pl.ds(h * N_BLK + j, 1), :]
            grow = jnp.exp(col(crow))
            grow = jnp.concatenate([grow, grow], axis=1)
            state = inc[h]
            cross = dot(qb, (prev[h * N_BLK + j] + state).astype(BF16))
            inc[h] = state * jnp.exp(crow[:, BLOCK - 1 : BLOCK])
            raw = inner[sl, h * DV : (h + 1) * DV] + cross * grow
            d = raw - jnp.mean(raw, axis=-1, keepdims=True)
            n = d * lax.rsqrt(jnp.mean(d * d, axis=-1, keepdims=True) + EPS)
            gate = silu(g_ref[sl, h * DV : (h + 1) * DV].astype(F32))
            ret[sl, h * DV : (h + 1) * DV] = (gate * n).astype(BF16)
        return 0

    sends = []
    lax.fori_loop(0, N_BLK, outer, 0)
    for d in (1, 2, 3):
        p = lax.rem(x + d, 4)
        cp = pltpu.make_async_remote_copy(
            src_ref=ret.at[rows(p * 512, 512), :],
            dst_ref=R.at[3 - d],
            send_sem=ret_s.at[d - 1],
            recv_sem=ret_r.at[d - 1],
            device_id=peer("tp", d),
            device_id_type=MESH,
        )
        cp.start()
        sends.append(cp)

    for cp in second_in:
        cp.wait_recv()
    own_half = c * 256
    other_half = (1 - c) * 256
    third = spread("ep_2", 1, own_half, 256, pl.ds(0, 2048), w3_s, w3_r)
    third.start()
    third_in = spread("ep_2", 1, other_half, 256, pl.ds(0, 2048), w3_s, w3_r)
    own_w.wait()
    for cp in sends:
        cp.wait_recv()
    third_in.wait_recv()

    def project(t, _):
        cols = pl.ds(pl.multiple_of(t * 512, 512), 512)
        acc = dot(ret[rows(x * 512, 512), :], W[0, :, cols])
        for g in (1, 2, 3):
            acc += dot(R[g - 1], W[g, :, cols])
        out_ref[:, cols] = acc.astype(BF16)
        return 0

    lax.fori_loop(0, 4, project, 0)
    for cp in first + second + sends + [third]:
        cp.wait_send()


def mixer_half(q, k, v, g, ld, wo):
    vm = pl.BlockSpec(memory_space=pltpu.VMEM)
    dma = pltpu.SemaphoreType.DMA
    return pl.pallas_call(
        mixer_kernel,
        name="mixer",
        out_shape=jax.ShapeDtypeStruct((512, 2048), BF16),
        in_specs=[vm, vm, vm, vm, vm, pl.BlockSpec(memory_space=pl.ANY)],
        out_specs=vm,
        scratch_shapes=[
            pltpu.VMEM((4, 512, 2048), BF16),
            pltpu.VMEM((3, 512, 512), BF16),
            pltpu.VMEM((2048, 512), BF16),
            pltpu.VMEM((2048, 512), F32),
            pltpu.VMEM((32, DK, DV), F32),
            pltpu.VMEM((32, BLOCK), F32),
            pltpu.VMEM((32, BLOCK), F32),
            pltpu.VMEM((32, BLOCK), F32),
            pltpu.VMEM((2, DK, DV), F32),
            pltpu.VMEM((2, DK, DV), F32),
            pltpu.VMEM((2, DK, DV), F32),
            pltpu.VMEM((2, 1, DV), F32),
            pltpu.VMEM((2, DK, DV), F32),
            pltpu.VMEM((2, 1, DV), F32),
            pltpu.VMEM((2, PAY, DV), BF16),
            pltpu.VMEM((1, 2, PAY, DV), BF16),
            pltpu.VMEM((3, 2, PAY, DV), BF16),
            pltpu.VMEM((3, 2, PAY, DV), BF16),
            dma((6,)), dma((6,)), dma((6,)), dma((6,)), dma((6,)), dma((6,)), dma, dma,
            dma((7,)), dma((7,)), dma((3,)), dma((3,)), dma,
        ],
        compiler_params=pltpu.CompilerParams(
            collective_id=0, has_side_effects=True, vmem_limit_bytes=50 * 1024 * 1024
        ),
        cost_estimate=pl.CostEstimate(flops=40_000_000_000, bytes_accessed=16_000_000, transcendentals=2_000_000),
    )(q, k, v, g, ld, wo)


N_TOK = 128
TOP = 4
CAP = 8
N_EP = 32
ROWS = N_EP * CAP
HALF = 1024


def moe_steps(ctx, x_ref, gain_ref, meta_ref, wg_hbm, wu_hbm, wd_hbm, sg_hbm, su_hbm, sd_hbm, out_ref, s):
    z, y, c, x = ctx.z, ctx.y, ctx.c, ctx.x
    start, mod = ctx.start, ctx.mod

    loads = []
    for i, (src, dst) in enumerate(
        ((sg_hbm, s.sg), (su_hbm, s.su), (sd_hbm, s.sd), (wg_hbm.at[0], s.wg), (wu_hbm.at[0], s.wu), (wd_hbm.at[0], s.wd))
    ):
        cp = pltpu.make_async_copy(src, dst, s.load.at[i])
        cp.start()
        loads.append(cp)

    v = x_ref[...].astype(F32)
    s.X[0] = (v * lax.rsqrt(jnp.mean(v * v, axis=-1, keepdims=True) + EPS) * gain_ref[...]).astype(BF16)
    s.meta[0] = meta_ref[...]
    gathers = {}
    sends = []
    for d in (1, 3, 2):
        a = start(s.meta.at[0], s.meta.at[4 - d], s.gm_s.at[d - 1], s.gm_r.at[d - 1], tp=d)
        b = start(s.X.at[0], s.X.at[4 - d], s.gx_s.at[d - 1], s.gx_r.at[d - 1], tp=d)
        gathers[4 - d] = (a, b)
        sends += [a, b]

    def build(gg):
        if gg:
            for cp in gathers[gg]:
                cp.wait_recv()
        rt = s.meta[gg, 0:TOP, :]
        wt = s.meta[gg, TOP : 2 * TOP, :]
        ident = (iota((N_EP, N_TOK), 0) * 4 + x).astype(F32)
        named = jnp.zeros((N_EP, N_TOK), F32)
        weight = jnp.zeros((N_EP, N_TOK), F32)
        for kk in range(TOP):
            hit = rt[kk : kk + 1, :] == ident
            named = named + jnp.where(hit, 1.0, 0.0)
            weight = weight + jnp.where(hit, wt[kk : kk + 1, :], 0.0)
        named = named.astype(BF16)
        earlier = (iota((N_TOK, N_TOK), 0) < iota((N_TOK, N_TOK), 1)).astype(F32).astype(BF16)
        rank = dot(named, earlier).astype(BF16)
        slot = iota((ROWS, N_EP), 0)
        spread = (slot // CAP == iota((ROWS, N_EP), 1)).astype(F32).astype(BF16)
        at = (iota((ROWS, N_TOK), 0) % CAP).astype(F32)
        live = (dot(spread, named) > 0.5) & (dot(spread, rank) == at)
        hi = weight.astype(BF16)
        lo = (weight - hi.astype(F32)).astype(BF16)
        s.whi[gg] = jnp.where(live, dot(spread, hi), 0.0).astype(BF16)
        s.wlo[gg] = jnp.where(live, dot(spread, lo), 0.0).astype(BF16)
        place = jnp.where(live, 1.0, 0.0).astype(BF16)
        for h in range(2):
            rows = dot(place, s.X[gg, :, h * HALF : (h + 1) * HALF]).astype(BF16)
            s.D[gg, h] = rows.reshape(4, 4, 2, CAP, HALF)
        s.M[gg, 0, z] = s.D[gg, 0, z]
        for zz in range(4):
            s.M[gg, 1, y, zz] = s.D[gg, 1, zz, y]
        for d in (1, 3, 2):
            zp, yp = mod(z + d), mod(y + d)
            first[gg, 0].append(
                start(s.D.at[gg, 0, zp], s.M.at[gg, 0, z], s.a_s.at[gg, 0, d - 1], s.a_r.at[gg, 0, d - 1], ep_0=d)
            )
            first[gg, 1].append(
                start(s.D.at[gg, 1, :, yp], s.M.at[gg, 1, y], s.a_s.at[gg, 1, d - 1], s.a_r.at[gg, 1, d - 1], ep_1=d)
            )

    first = {(gg, h): [] for gg in range(4) for h in range(2)}
    second = {(gg, h): [] for gg in range(4) for h in range(2)}
    third = {(gg, h): [] for gg in range(4) for h in range(2)}
    fourth = {(gg, h): [] for gg in range(4) for h in range(2)}
    hops = [(1, 0), (3, 0), (1, 1), (3, 1), (2, 0), (2, 1), (0, 1)]

    def relay(gg):
        for h in range(2):
            for cp in first[gg, h]:
                cp.wait_recv()
            for i, (d, e) in enumerate(hops):
                zp, yp, cp_ = mod(z + d), mod(y + d), lax.rem(c + e, 2)
                if h == 0:
                    src, dst = s.M.at[gg, 0, :, yp, cp_], s.V.at[gg, 0, :, y, c]
                    to = {"ep_1": d, "ep_2": e}
                else:
                    src, dst = s.M.at[gg, 1, :, zp, cp_], s.V.at[gg, 1, z, :, c]
                    to = {"ep_0": d, "ep_2": e}
                second[gg, h].append(start(src, dst, s.b_s.at[gg, h, i], s.b_r.at[gg, h, i], **to))
            for k in range(4):
                if h == 0:
                    s.V[gg, 0, k, y, c] = s.M[gg, 0, k, y, c]
                else:
                    s.V[gg, 1, z, k, c] = s.M[gg, 1, k, z, c]

    def expert(gg):
        for h in range(2):
            for cp in second[gg, h]:
                cp.wait_recv()
        a = s.V[gg, 0].reshape(ROWS, HALF)
        b = s.V[gg, 1].reshape(ROWS, HALF)
        gate = dot(a, s.wg[0:HALF]) + dot(b, s.wg[HALF:])
        up = dot(a, s.wu[0:HALF]) + dot(b, s.wu[HALF:])
        hidden = (silu(gate) * up).astype(BF16)
        for h in range(2):
            rows = dot(hidden, s.wd[:, h * HALF : (h + 1) * HALF]).astype(BF16)
            s.V[gg, h] = rows.reshape(4, 4, 2, CAP, HALF)

    def give_back(gg):
        for h in range(2):
            for i, (d, e) in enumerate(hops):
                zp, yp, cp_ = mod(z + d), mod(y + d), lax.rem(c + e, 2)
                if h == 0:
                    src, dst = s.V.at[gg, 0, :, yp, cp_], s.N.at[gg, 0, :, y, c]
                    to = {"ep_1": d, "ep_2": e}
                else:
                    src, dst = s.V.at[gg, 1, zp, :, cp_], s.N.at[gg, 1, :, z, c]
                    to = {"ep_0": d, "ep_2": e}
                third[gg, h].append(start(src, dst, s.c_s.at[gg, h, i], s.c_r.at[gg, h, i], **to))
            for k in range(4):
                if h == 0:
                    s.N[gg, 0, k, y, c] = s.V[gg, 0, k, y, c]
                else:
                    s.N[gg, 1, k, z, c] = s.V[gg, 1, z, k, c]

    def relay_back(gg):
        for h in range(2):
            for cp in third[gg, h]:
                cp.wait_recv()
            for d in (1, 3, 2):
                zp, yp = mod(z + d), mod(y + d)
                if h == 0:
                    cp = start(s.N.at[gg, 0, zp], s.B.at[gg, 0, z], s.d_s.at[gg, 0, d - 1], s.d_r.at[gg, 0, d - 1], ep_0=d)
                else:
                    cp = start(s.N.at[gg, 1, yp], s.B.at[gg, 1, :, y], s.d_s.at[gg, 1, d - 1], s.d_r.at[gg, 1, d - 1], ep_1=d)
                fourth[gg, h].append(cp)
            if h == 0:
                s.B[gg, 0, z] = s.N[gg, 0, z]
            else:
                for zz in range(4):
                    s.B[gg, 1, zz, y] = s.N[gg, 1, y, zz]

    reduces = {}

    def fold(gg):
        for h in range(2):
            cols = slice(h * HALF, (h + 1) * HALF)
            for cp in fourth[gg, h]:
                cp.wait_recv()
            back = s.B[gg, h].reshape(ROWS, HALF)
            part = dot(s.whi[gg], back, TN) + dot(s.wlo[gg], back, TN)
            if gg == 0:
                s.acc[:, cols] = s.acc[:, cols] + part
            else:
                s.P[gg - 1, h] = part.astype(BF16)
                reduces[gg, h] = start(
                    s.P.at[gg - 1, h], s.G.at[gg - 1, h], s.e_s.at[gg - 1, h], s.e_r.at[gg - 1, h], tp=gg
                )

    def shared():
        for cp in loads[:3]:
            cp.wait()
        rows = s.X[0]
        hidden = (silu(dot(rows, s.sg[...])) * dot(rows, s.su[...])).astype(BF16)
        for h in range(2):
            cols = slice(h * HALF, (h + 1) * HALF)
            s.acc[:, cols] = dot(hidden, s.sd[:, cols])

    def finish():
        for h in range(2):
            cols = slice(h * HALF, (h + 1) * HALF)
            total = s.acc[:, cols]
            for gg in (1, 2, 3):
                reduces[gg, h].wait_recv()
                total = total + s.G[gg - 1, h].astype(F32)
            out_ref[:, cols] = total.astype(BF16)
        for group in (first, second, third, fourth):
            for cps in group.values():
                for cp in cps:
                    cp.wait_send()
        for cp in list(reduces.values()) + sends:
            cp.wait_send()

    def weights():
        for cp in loads[3:]:
            cp.wait()

    return dict(
        build=build, relay=relay, expert=expert, give_back=give_back, relay_back=relay_back,
        fold=fold, shared=shared, finish=finish, weights=weights,
    )


class Names:
    pass


class Ctx:
    def __init__(self):
        self.z = lax.axis_index("ep_0")
        self.y = lax.axis_index("ep_1")
        self.c = lax.axis_index("ep_2")
        self.x = lax.axis_index("tp")
        self.place = {"ep_0": self.z, "ep_1": self.y, "ep_2": self.c, "tp": self.x}
        self.size = {"ep_0": 4, "ep_1": 4, "ep_2": 2, "tp": 4}

    def mod(self, v):
        return lax.rem(v, 4)

    def peer(self, **offsets):
        return {a: lax.rem(self.place[a] + d, self.size[a]) for a, d in offsets.items() if d}

    def copy(self, src, dst, send, recv, **offsets):
        return pltpu.make_async_remote_copy(
            src_ref=src, dst_ref=dst, send_sem=send, recv_sem=recv,
            device_id=self.peer(**offsets), device_id_type=MESH,
        )

    def start(self, src, dst, send, recv, **offsets):
        cp = self.copy(src, dst, send, recv, **offsets)
        cp.start()
        return cp


def greet(ctx):
    peers = [dict(tp=d) for d in (1, 2, 3)]
    peers += [dict(ep_0=d, ep_2=e) for d in (1, 2, 3) for e in (0, 1)]
    peers += [dict(ep_1=d, ep_2=e) for d in (1, 2, 3) for e in (0, 1)]
    peers += [dict(ep_2=1)]
    barrier = pltpu.get_barrier_semaphore()
    for p in peers:
        pl.semaphore_signal(barrier, inc=1, device_id=ctx.peer(**p), device_id_type=MESH)
    pl.semaphore_wait(barrier, len(peers))


DMA = pltpu.SemaphoreType.DMA
BLK = (4, 4, 2, CAP, HALF)
MOE_SCRATCH = dict(
    sg=pltpu.VMEM((2048, 512), BF16), su=pltpu.VMEM((2048, 512), BF16), sd=pltpu.VMEM((512, 2048), BF16),
    wg=pltpu.VMEM((2048, 512), BF16), wu=pltpu.VMEM((2048, 512), BF16), wd=pltpu.VMEM((512, 2048), BF16),
    X=pltpu.VMEM((4, N_TOK, 2048), BF16), meta=pltpu.VMEM((4, 8, N_TOK), F32),
    whi=pltpu.VMEM((4, ROWS, N_TOK), BF16), wlo=pltpu.VMEM((4, ROWS, N_TOK), BF16),
    D=pltpu.VMEM((4, 2) + BLK, BF16), M=pltpu.VMEM((4, 2) + BLK, BF16), V=pltpu.VMEM((4, 2) + BLK, BF16),
    N=pltpu.VMEM((4, 2) + BLK, BF16), B=pltpu.VMEM((4, 2) + BLK, BF16),
    acc=pltpu.VMEM((N_TOK, 2048), F32),
    P=pltpu.VMEM((3, 2, N_TOK, HALF), BF16), G=pltpu.VMEM((3, 2, N_TOK, HALF), BF16),
    load=DMA((6,)),
    gm_s=DMA((3,)), gm_r=DMA((3,)), gx_s=DMA((3,)), gx_r=DMA((3,)),
    a_s=DMA((4, 2, 3)), a_r=DMA((4, 2, 3)), b_s=DMA((4, 2, 7)), b_r=DMA((4, 2, 7)),
    c_s=DMA((4, 2, 7)), c_r=DMA((4, 2, 7)), d_s=DMA((4, 2, 3)), d_r=DMA((4, 2, 3)),
    e_s=DMA((3, 2)), e_r=DMA((3, 2)),
)


def moe_kernel(x_ref, gain_ref, meta_ref, wg, wu, wd, sg, su, sd, out_ref, *scratch):
    ctx = Ctx()
    s = Names()
    for name, ref in zip(MOE_SCRATCH, scratch):
        setattr(s, name, ref)
    greet(ctx)
    m = moe_steps(ctx, x_ref, gain_ref, meta_ref, wg, wu, wd, sg, su, sd, out_ref, s)
    m["build"](0)
    m["shared"]()
    m["build"](1)
    m["relay"](0)
    m["build"](3)
    m["relay"](1)
    m["weights"]()
    m["expert"](0)
    m["build"](2)
    m["relay"](3)
    m["expert"](1)
    m["give_back"](1)
    m["relay"](2)
    m["expert"](3)
    m["give_back"](3)
    m["relay_back"](1)
    m["expert"](2)
    m["give_back"](2)
    m["relay_back"](3)
    m["give_back"](0)
    m["fold"](1)
    m["relay_back"](2)
    m["fold"](3)
    m["relay_back"](0)
    m["fold"](2)
    m["fold"](0)
    m["finish"]()


def moe_half(x, gain, routing, weight, wg, wu, wd, sg, su, sd):
    meta = jnp.concatenate([routing.T.astype(F32), weight.T], axis=0)
    vm = pl.BlockSpec(memory_space=pltpu.VMEM)
    hbm = pl.BlockSpec(memory_space=pl.ANY)
    return pl.pallas_call(
        moe_kernel,
        name="moe",
        out_shape=jax.ShapeDtypeStruct((N_TOK, 2048), BF16),
        in_specs=[vm, vm, vm] + [hbm] * 6,
        out_specs=vm,
        scratch_shapes=list(MOE_SCRATCH.values()),
        compiler_params=pltpu.CompilerParams(
            collective_id=1, has_side_effects=True, vmem_limit_bytes=60 * 1024 * 1024
        ),
        cost_estimate=pl.CostEstimate(flops=9_000_000_000, bytes_accessed=16_000_000, transcendentals=0),
    )(x, gain.reshape(1, -1), meta, wg, wu, wd, sg, su, sd)


def local(
    query_rows, key_rows, value_rows, gate_rows, log_decay, out_proj,
    moe_input, norm_gain, routing, route_weight,
    expert_gate, expert_up, expert_down, shared_gate, shared_up, shared_down,
):
    mixer_out = mixer_half(query_rows, key_rows, value_rows, gate_rows, log_decay, out_proj)
    moe_out = moe_half(
        moe_input, norm_gain, routing, route_weight,
        expert_gate, expert_up, expert_down, shared_gate, shared_up, shared_down,
    )
    return (mixer_out, moe_out)


def solution(mesh):
    split = Mesh(mesh.devices.reshape(4, 4, 2, mesh.shape["tp"]), ("ep_0", "ep_1", "ep_2", "tp"))
    return jax.shard_map(
        local,
        mesh=split,
        in_specs=(
            P(EP, "tp"),
            P(EP, "tp"),
            P(EP, "tp"),
            P(EP, "tp"),
            P("tp", EP),
            P("tp", None),
            P(EP_TP, None),
            P(),
            P(EP_TP, None),
            P(EP_TP, None),
            P(EP_TP, None, None),
            P(EP_TP, None, None),
            P(EP_TP, None, None),
            P(),
            P(),
            P(),
        ),
        out_specs=(P(EP_TP, None), P(EP_TP, None)),
        check_vma=False,
    )
```

```python
import functools

import jax
import jax.numpy as jnp
from jax import lax
from jax.experimental import pallas as pl
from jax.experimental.pallas import tpu as pltpu
from jax.sharding import Mesh
from jax.sharding import PartitionSpec as P

DK = 128
DV = 256
BLOCK = 128
EP = ("ep_0", "ep_1", "ep_2")
EP_TP = ("ep_0", "ep_1", "ep_2", "tp")
EPS = 1e-06
MESH = pl.DeviceIdType.MESH
HI = lax.Precision.HIGHEST
F32 = jnp.float32
BF16 = jnp.bfloat16
SCALE = DK ** (-0.5)

NT = (((1,), (1,)), ((), ()))
TN = (((0,), (0,)), ((), ()))


def dot(a, b, dims=None, precision=None):
    if dims is None:
        dims = (((1,), (0,)), ((), ()))
    return lax.dot_general(a, b, dims, precision=precision, preferred_element_type=F32)


def iota(shape, dim):
    return lax.broadcasted_iota(jnp.int32, shape, dim)


def silu(v):
    half = 0.5 * v
    return half * jnp.tanh(half) + half


N_BLK = 16
HEADS = 2
PAY = DK + 16


def mixer_steps(ctx, q_hbm, k_hbm, v_hbm, g_hbm, ld_ref, wo_ref, out_ref, s):
    z, y, c, x = ctx.z, ctx.y, ctx.c, ctx.x
    start, copy, mod = ctx.start, ctx.copy, ctx.mod
    nb = HEADS * N_BLK

    def rows(first, n):
        return pl.ds(pl.multiple_of(first, 16), n)

    whole = pl.ds(0, 2048)
    direct, half0, half1 = pl.ds(0, 1024), pl.ds(1024, 512), pl.ds(1536, 512)
    r0 = c * 256 + y * 64 + z * 16
    r1 = c * 256 + z * 64 + y * 16
    loads = {}

    def fetch():
        for i, (name, src, dst) in enumerate(
            (("k", k_hbm, s.k), ("v", v_hbm, s.v), ("q", q_hbm, s.q), ("g", g_hbm, s.g), ("w", wo_ref, s.W.at[0]))
        ):
            loads[name] = pltpu.make_async_copy(src, dst, s.in_sem.at[i])
            loads[name].start()

    wx, wd = [], []

    def spread_x():
        for d in (1, 3, 2):
            for h, (r, cols) in enumerate(((r0, half0), (r1, half1))):
                i = (d - 1) * 2 + h
                wx.append(
                    start(wo_ref.at[rows(r, 16), cols], s.W.at[4 - d, rows(r, 16), cols], s.wx_s.at[i], s.wx_r.at[i], tp=d)
                )
        for d in (1, 3, 2):
            r = rows(c * 256, 256)
            wd.append(start(wo_ref.at[r, direct], s.W.at[4 - d, r, direct], s.wd_s.at[d - 1], s.wd_r.at[d - 1], tp=d))

    def decays():
        for h in range(HEADS):
            for j in range(N_BLK):
                s.a[h * N_BLK + j : h * N_BLK + j + 1, :] = ld_ref[h : h + 1, j * BLOCK : (j + 1) * BLOCK]
        upper = (iota((BLOCK, BLOCK), 0) <= iota((BLOCK, BLOCK), 1)).astype(F32)
        cum = dot(s.a[...], upper, precision=HI)
        s.cum[...] = cum
        totb = jnp.broadcast_to(cum[:, BLOCK - 1 : BLOCK], (nb, BLOCK))
        ri, ci = iota((nb, nb), 0), iota((nb, nb), 1)
        same = (ri // N_BLK) == (ci // N_BLK)
        after = dot((same & (ci > ri)).astype(F32), totb, precision=HI)
        ahead = dot((same & (ci < ri)).astype(F32), totb, precision=HI)
        s.e[...] = jnp.exp(after + totb - cum) * SCALE
        s.fac[...] = jnp.exp(ahead)
        full = jnp.exp(after + totb)
        s.run[...] = jnp.zeros_like(s.run)
        for h in range(HEADS):
            f = full[h * N_BLK : h * N_BLK + 1, :]
            s.tot_f[h] = jnp.concatenate([f, f], axis=1)

    def col(row):
        return jnp.broadcast_to(row, (BLOCK, BLOCK)).T

    def block(j):
        return pl.ds(pl.multiple_of(j * BLOCK, BLOCK), BLOCK)

    def summary():
        loads["k"].wait()
        loads["v"].wait()

        def body(j, _):
            sl = block(j)
            for h in range(HEADS):
                kb = s.k[sl, h * DK : (h + 1) * DK].astype(F32)
                vb = s.v[sl, h * DV : (h + 1) * DV]
                kd = (kb * col(s.e[pl.ds(h * N_BLK + j, 1), :])).astype(BF16)
                s.run[h] += dot(kd, vb, TN)
            return 0

        lax.fori_loop(0, N_BLK, body, 0)
        for h in range(HEADS):
            s.tot_S[h] = s.run[h]
            s.bef_S[h] = jnp.zeros((DK, DV), F32)
            s.bef_f[h] = jnp.ones((1, DV), F32)
        s.run[...] = jnp.zeros_like(s.run)
        loads["q"].wait()

    states = {"ep_2": (s.got_c, 0), "ep_1": (s.got_y, 1), "ep_0": (s.got_z, 4)}
    flying = {}

    def publish(axis):
        got, base = states[axis]
        for h in range(HEADS):
            s.pay[base and 1 + base // 4, h, 0:DK, :] = s.tot_S[h].astype(BF16)
            f = s.tot_f[h]
            f1 = f.astype(BF16)
            f2 = (f - f1.astype(F32)).astype(BF16)
            row = iota((16, DV), 0)
            top = jnp.where(row == 0, f1.astype(F32), jnp.where(row == 1, f2.astype(F32), 0.0))
            s.pay[base and 1 + base // 4, h, DK:PAY, :] = top.astype(BF16)
        flying[axis] = [
            start(
                s.pay.at[base and 1 + base // 4], got.at[d - 1],
                s.pre_s.at[base + d - 1], s.pre_r.at[base + d - 1], **{axis: d}
            )
            for d in range(1, ctx.size[axis])
        ]

    def absorb(axis):
        got, _ = states[axis]
        n, at = ctx.size[axis], ctx.place[axis]
        for cp in flying[axis]:
            cp.wait_recv()
        for h in range(HEADS):
            sub_f = jnp.ones((1, DV), F32)
            sub_S = jnp.zeros((DK, DV), F32)
            in_f, in_S = sub_f, sub_S
            for kk in range(n):
                own = at == kk
                slot = jnp.maximum(lax.rem(at - kk + n, n) - 1, 0)
                piece = got[slot, h].astype(F32)
                pf = piece[DK : DK + 1, :] + piece[DK + 1 : DK + 2, :]
                pf = jnp.where(own, s.tot_f[h], pf)
                ps = jnp.where(own, s.tot_S[h], piece[0:DK, :])
                if kk:
                    in_f = jnp.where(own, sub_f, in_f)
                    in_S = jnp.where(own, sub_S, in_S)
                sub_S = pf * sub_S + ps
                sub_f = sub_f * pf
            s.bef_S[h] = s.bef_f[h] * in_S + s.bef_S[h]
            s.bef_f[h] = s.bef_f[h] * in_f
            s.tot_S[h] = sub_S
            s.tot_f[h] = sub_f

    def inside(lo, hi):
        causal = iota((BLOCK, BLOCK), 0) >= iota((BLOCK, BLOCK), 1)

        def body(j, _):
            sl = block(j)
            for h in range(HEADS):
                qb = s.q[sl, h * DK : (h + 1) * DK]
                kb = s.k[sl, h * DK : (h + 1) * DK]
                vb = s.v[sl, h * DV : (h + 1) * DV]
                crow = s.cum[pl.ds(h * N_BLK + j, 1), :]
                ccol = col(crow)
                gap = ccol - jnp.broadcast_to(crow, (BLOCK, BLOCK))
                dec = jnp.exp(jnp.where(causal, gap, -1e30)) * SCALE
                w = (dot(qb, kb, NT) * dec).astype(BF16)
                s.inner[sl, h * DV : (h + 1) * DV] = dot(w, vb)
                last = crow[:, BLOCK - 1 : BLOCK]
                kd = (kb.astype(F32) * (jnp.exp(last - ccol) * SCALE)).astype(BF16)
                s.prev[h * N_BLK + j] = s.run[h].astype(BF16)
                s.run[h] = s.run[h] * jnp.exp(last) + dot(kd, vb, TN)
            return 0

        lax.fori_loop(lo, hi, body, 0)

    def near(axis, d, r, n, cols, ss, rs):
        ref = s.W.at[1:4, rows(r, n), cols]
        return copy(ref, ref, ss, rs, **{axis: d})

    def ring(n, plan, ss, rs, out, into):
        for d in (1, 3, 2):
            for h, (axis, mine, theirs, cols) in enumerate(plan):
                i = (d - 1) * 2 + h
                cp = near(axis, d, mine, n, cols, ss.at[i], rs.at[i])
                cp.start()
                out.append(cp)
                into.append(near(axis, d, theirs(d), n, cols, ss.at[i], rs.at[i]))

    first, first_in, second, second_in, third = [], [], [], [], []

    def spread_1():
        for cp in wx:
            cp.wait_recv()
        ring(
            16,
            (
                ("ep_0", r0, lambda d: c * 256 + y * 64 + mod(z + 4 - d) * 16, half0),
                ("ep_1", r1, lambda d: c * 256 + z * 64 + mod(y + 4 - d) * 16, half1),
            ),
            s.w1_s, s.w1_r, first, first_in,
        )

    def spread_2():
        for cp in first_in:
            cp.wait_recv()
        ring(
            64,
            (
                ("ep_1", c * 256 + y * 64, lambda d: c * 256 + mod(y + 4 - d) * 64, half0),
                ("ep_0", c * 256 + z * 64, lambda d: c * 256 + mod(z + 4 - d) * 64, half1),
            ),
            s.w2_s, s.w2_r, second, second_in,
        )

    def spread_3():
        for cp in second_in + wd:
            cp.wait_recv()
        cp = near("ep_2", 1, c * 256, 256, whole, s.w3_s, s.w3_r)
        cp.start()
        third.extend([cp, near("ep_2", 1, (1 - c) * 256, 256, whole, s.w3_s, s.w3_r)])

    sends = {}

    def outer(d):
        p = mod(x + d)

        def body(i, _):
            j = p * 4 + i
            sl = block(j)
            for h in range(HEADS):
                qb = s.q[sl, h * DK : (h + 1) * DK]
                crow = s.cum[pl.ds(h * N_BLK + j, 1), :]
                grow = jnp.exp(col(crow))
                grow = jnp.concatenate([grow, grow], axis=1)
                fac = s.fac[pl.ds(h * N_BLK + j, 1), :]
                fac = jnp.concatenate([fac, fac], axis=1)
                state = s.prev[h * N_BLK + j].astype(F32) + s.bef_S[h] * fac
                cross = dot(qb, state.astype(BF16))
                raw = s.inner[sl, h * DV : (h + 1) * DV] + cross * grow
                dev = raw - jnp.mean(raw, axis=-1, keepdims=True)
                n = dev * lax.rsqrt(jnp.mean(dev * dev, axis=-1, keepdims=True) + EPS)
                gate = silu(s.g[sl, h * DV : (h + 1) * DV].astype(F32))
                s.g[sl, h * DV : (h + 1) * DV] = (gate * n).astype(BF16)
            return 0

        lax.fori_loop(0, 4, body, 0)
        if d:
            sends[d] = start(
                s.g.at[rows(p * 512, 512), :], s.R.at[3 - d], s.ret_s.at[d - 1], s.ret_r.at[d - 1], tp=d
            )

    def ready():
        loads["w"].wait()
        for cp in sends.values():
            cp.wait_recv()
        third[1].wait_recv()

    def project(lo, hi):
        def body(t, _):
            cols = pl.ds(pl.multiple_of(t * 512, 512), 512)
            acc = dot(s.g[rows(x * 512, 512), :], s.W[0, :, cols])
            for g in (1, 2, 3):
                acc += dot(s.R[g - 1], s.W[g, :, cols])
            out_ref[:, cols] = acc.astype(BF16)
            return 0

        lax.fori_loop(lo, hi, body, 0)

    def finish():
        for cp in wx + wd + first + second + third[:1] + list(sends.values()) + sum(flying.values(), []):
            cp.wait_send()

    def gate_in():
        loads["g"].wait()

    return dict(
        fetch=fetch, spread_x=spread_x, decays=decays, summary=summary, publish=publish, absorb=absorb, inside=inside,
        spread_1=spread_1, spread_2=spread_2, spread_3=spread_3, outer=outer, ready=ready, project=project,
        finish=finish, gate_in=gate_in,
    )


N_TOK = 128
TOP = 4
CAP = 8
N_EP = 32
ROWS = N_EP * CAP
HALF = 1024


def moe_steps(ctx, x_ref, gain_ref, meta_ref, wg_hbm, wu_hbm, wd_hbm, sg_hbm, su_hbm, sd_hbm, out_ref, s):
    z, y, c, x = ctx.z, ctx.y, ctx.c, ctx.x
    start, mod = ctx.start, ctx.mod

    def fetch(first, *sources):
        for i, (src, dst) in enumerate(zip(sources, (s.wg, s.wu, s.wd))):
            cp = pltpu.make_async_copy(src, dst, s.load.at[first + i])
            cp.start()
            loads.append(cp)

    loads = []
    fetch(0, sg_hbm, su_hbm, sd_hbm)

    v = x_ref[...].astype(F32)
    s.X[0] = (v * lax.rsqrt(jnp.mean(v * v, axis=-1, keepdims=True) + EPS) * gain_ref[...]).astype(BF16)
    s.meta[0] = meta_ref[...]
    gathers = {}
    sends = []
    for d in (1, 3, 2):
        a = start(s.meta.at[0], s.meta.at[4 - d], s.gm_s.at[d - 1], s.gm_r.at[d - 1], tp=d)
        b = start(s.X.at[0], s.X.at[4 - d], s.gx_s.at[d - 1], s.gx_r.at[d - 1], tp=d)
        gathers[4 - d] = (a, b)
        sends += [a, b]

    def build(gg):
        if gg:
            for cp in gathers[gg]:
                cp.wait_recv()
        rt = s.meta[gg, 0:TOP, :]
        wt = s.meta[gg, TOP : 2 * TOP, :]
        ident = (iota((N_EP, N_TOK), 0) * 4 + x).astype(F32)
        named = jnp.zeros((N_EP, N_TOK), F32)
        weight = jnp.zeros((N_EP, N_TOK), F32)
        for kk in range(TOP):
            hit = rt[kk : kk + 1, :] == ident
            named = named + jnp.where(hit, 1.0, 0.0)
            weight = weight + jnp.where(hit, wt[kk : kk + 1, :], 0.0)
        named = named.astype(BF16)
        earlier = (iota((N_TOK, N_TOK), 0) < iota((N_TOK, N_TOK), 1)).astype(F32).astype(BF16)
        rank = dot(named, earlier).astype(BF16)
        slot = iota((ROWS, N_EP), 0)
        spread = (slot // CAP == iota((ROWS, N_EP), 1)).astype(F32).astype(BF16)
        at = (iota((ROWS, N_TOK), 0) % CAP).astype(F32)
        live = (dot(spread, named) > 0.5) & (dot(spread, rank) == at)
        hi = weight.astype(BF16)
        lo = (weight - hi.astype(F32)).astype(BF16)
        s.whi[gg] = jnp.where(live, dot(spread, hi), 0.0).astype(BF16)
        s.wlo[gg] = jnp.where(live, dot(spread, lo), 0.0).astype(BF16)
        place = jnp.where(live, 1.0, 0.0).astype(BF16)
        for h in range(2):
            rows = dot(place, s.X[gg, :, h * HALF : (h + 1) * HALF]).astype(BF16)
            s.D[gg, h] = rows.reshape(4, 4, 2, CAP, HALF)
        s.M[gg, 0, z] = s.D[gg, 0, z]
        for zz in range(4):
            s.M[gg, 1, y, zz] = s.D[gg, 1, zz, y]
        for d in (1, 3, 2):
            zp, yp = mod(z + d), mod(y + d)
            first[gg, 0].append(
                start(s.D.at[gg, 0, zp], s.M.at[gg, 0, z], s.a_s.at[gg, 0, d - 1], s.a_r.at[gg, 0, d - 1], ep_0=d)
            )
            first[gg, 1].append(
                start(s.D.at[gg, 1, :, yp], s.M.at[gg, 1, y], s.a_s.at[gg, 1, d - 1], s.a_r.at[gg, 1, d - 1], ep_1=d)
            )

    first = {(gg, h): [] for gg in range(4) for h in range(2)}
    second = {(gg, h): [] for gg in range(4) for h in range(2)}
    third = {(gg, h): [] for gg in range(4) for h in range(2)}
    fourth = {(gg, h): [] for gg in range(4) for h in range(2)}
    hops = [(1, 0), (3, 0), (1, 1), (3, 1), (2, 0), (2, 1), (0, 1)]

    def relay(gg):
        for h in range(2):
            for cp in first[gg, h]:
                cp.wait_recv()
            for i, (d, e) in enumerate(hops):
                zp, yp, cp_ = mod(z + d), mod(y + d), lax.rem(c + e, 2)
                if h == 0:
                    src, dst = s.M.at[gg, 0, :, yp, cp_], s.V.at[gg, 0, :, y, c]
                    to = {"ep_1": d, "ep_2": e}
                else:
                    src, dst = s.M.at[gg, 1, :, zp, cp_], s.V.at[gg, 1, z, :, c]
                    to = {"ep_0": d, "ep_2": e}
                second[gg, h].append(start(src, dst, s.b_s.at[gg, h, i], s.b_r.at[gg, h, i], **to))
            for k in range(4):
                if h == 0:
                    s.V[gg, 0, k, y, c] = s.M[gg, 0, k, y, c]
                else:
                    s.V[gg, 1, z, k, c] = s.M[gg, 1, k, z, c]

    def expert(gg):
        for h in range(2):
            for cp in second[gg, h]:
                cp.wait_recv()
        a = s.V[gg, 0].reshape(ROWS, HALF)
        b = s.V[gg, 1].reshape(ROWS, HALF)
        gate = dot(a, s.wg[0:HALF]) + dot(b, s.wg[HALF:])
        up = dot(a, s.wu[0:HALF]) + dot(b, s.wu[HALF:])
        hidden = (silu(gate) * up).astype(BF16)
        for h in range(2):
            rows = dot(hidden, s.wd[:, h * HALF : (h + 1) * HALF]).astype(BF16)
            s.V[gg, h] = rows.reshape(4, 4, 2, CAP, HALF)

    def give_back(gg):
        for h in range(2):
            for i, (d, e) in enumerate(hops):
                zp, yp, cp_ = mod(z + d), mod(y + d), lax.rem(c + e, 2)
                if h == 0:
                    src, dst = s.V.at[gg, 0, :, yp, cp_], s.N.at[gg, 0, :, y, c]
                    to = {"ep_1": d, "ep_2": e}
                else:
                    src, dst = s.V.at[gg, 1, zp, :, cp_], s.N.at[gg, 1, :, z, c]
                    to = {"ep_0": d, "ep_2": e}
                third[gg, h].append(start(src, dst, s.c_s.at[gg, h, i], s.c_r.at[gg, h, i], **to))
            for k in range(4):
                if h == 0:
                    s.N[gg, 0, k, y, c] = s.V[gg, 0, k, y, c]
                else:
                    s.N[gg, 1, k, z, c] = s.V[gg, 1, z, k, c]

    def relay_back(gg):
        for h in range(2):
            for cp in third[gg, h]:
                cp.wait_recv()
            for d in (1, 3, 2):
                zp, yp = mod(z + d), mod(y + d)
                if h == 0:
                    cp = start(s.N.at[gg, 0, zp], s.B.at[gg, 0, z], s.d_s.at[gg, 0, d - 1], s.d_r.at[gg, 0, d - 1], ep_0=d)
                else:
                    cp = start(s.N.at[gg, 1, yp], s.B.at[gg, 1, :, y], s.d_s.at[gg, 1, d - 1], s.d_r.at[gg, 1, d - 1], ep_1=d)
                fourth[gg, h].append(cp)
            if h == 0:
                s.B[gg, 0, z] = s.N[gg, 0, z]
            else:
                for zz in range(4):
                    s.B[gg, 1, zz, y] = s.N[gg, 1, y, zz]

    reduces = {}

    def fold(gg):
        for h in range(2):
            cols = slice(h * HALF, (h + 1) * HALF)
            for cp in fourth[gg, h]:
                cp.wait_recv()
            back = s.B[gg, h].reshape(ROWS, HALF)
            part = dot(s.whi[gg], back, TN) + dot(s.wlo[gg], back, TN)
            if gg == 0:
                s.acc[:, cols] = s.acc[:, cols] + part
            else:
                s.P[gg - 1, h] = part.astype(BF16)
                reduces[gg, h] = start(
                    s.P.at[gg - 1, h], s.G.at[gg - 1, h], s.e_s.at[gg - 1, h], s.e_r.at[gg - 1, h], tp=gg
                )

    def shared():
        for cp in loads[:3]:
            cp.wait()
        rows = s.X[0]
        hidden = (silu(dot(rows, s.wg[...])) * dot(rows, s.wu[...])).astype(BF16)
        for h in range(2):
            cols = slice(h * HALF, (h + 1) * HALF)
            s.acc[:, cols] = dot(hidden, s.wd[:, cols])
        fetch(3, wg_hbm.at[0], wu_hbm.at[0], wd_hbm.at[0])

    def finish():
        for h in range(2):
            cols = slice(h * HALF, (h + 1) * HALF)
            total = s.acc[:, cols]
            for gg in (1, 2, 3):
                reduces[gg, h].wait_recv()
                total = total + s.G[gg - 1, h].astype(F32)
            out_ref[:, cols] = total.astype(BF16)
        for group in (first, second, third, fourth):
            for cps in group.values():
                for cp in cps:
                    cp.wait_send()
        for cp in list(reduces.values()) + sends:
            cp.wait_send()

    def weights():
        for cp in loads[3:]:
            cp.wait()

    return dict(
        build=build, relay=relay, expert=expert, give_back=give_back, relay_back=relay_back,
        fold=fold, shared=shared, finish=finish, weights=weights,
    )


class Names:
    pass


class Ctx:
    def __init__(self):
        self.z = lax.axis_index("ep_0")
        self.y = lax.axis_index("ep_1")
        self.c = lax.axis_index("ep_2")
        self.x = lax.axis_index("tp")
        self.place = {"ep_0": self.z, "ep_1": self.y, "ep_2": self.c, "tp": self.x}
        self.size = {"ep_0": 4, "ep_1": 4, "ep_2": 2, "tp": 4}

    def mod(self, v):
        return lax.rem(v, 4)

    def peer(self, **offsets):
        return {a: lax.rem(self.place[a] + d, self.size[a]) for a, d in offsets.items() if d}

    def copy(self, src, dst, send, recv, **offsets):
        return pltpu.make_async_remote_copy(
            src_ref=src, dst_ref=dst, send_sem=send, recv_sem=recv,
            device_id=self.peer(**offsets), device_id_type=MESH,
        )

    def start(self, src, dst, send, recv, **offsets):
        cp = self.copy(src, dst, send, recv, **offsets)
        cp.start()
        return cp


def greet(ctx):
    peers = [dict(tp=d) for d in (1, 2, 3)]
    peers += [dict(ep_0=d, ep_2=e) for d in (1, 2, 3) for e in (0, 1)]
    peers += [dict(ep_1=d, ep_2=e) for d in (1, 2, 3) for e in (0, 1)]
    peers += [dict(ep_2=1)]
    barrier = pltpu.get_barrier_semaphore()
    for p in peers:
        pl.semaphore_signal(barrier, inc=1, device_id=ctx.peer(**p), device_id_type=MESH)
    pl.semaphore_wait(barrier, len(peers))


DMA = pltpu.SemaphoreType.DMA
BLK = (4, 4, 2, CAP, HALF)
SCRATCH = dict(
    wg=pltpu.VMEM((2048, 512), BF16), wu=pltpu.VMEM((2048, 512), BF16), wd=pltpu.VMEM((512, 2048), BF16),
    X=pltpu.VMEM((4, N_TOK, 2048), BF16), meta=pltpu.VMEM((4, 8, N_TOK), F32),
    whi=pltpu.VMEM((4, ROWS, N_TOK), BF16), wlo=pltpu.VMEM((4, ROWS, N_TOK), BF16),
    D=pltpu.VMEM((4, 2) + BLK, BF16), M=pltpu.VMEM((4, 2) + BLK, BF16), V=pltpu.VMEM((4, 2) + BLK, BF16),
    N=pltpu.VMEM((4, 2) + BLK, BF16), B=pltpu.VMEM((4, 2) + BLK, BF16),
    acc=pltpu.VMEM((N_TOK, 2048), F32),
    P=pltpu.VMEM((3, 2, N_TOK, HALF), BF16), G=pltpu.VMEM((3, 2, N_TOK, HALF), BF16),
    load=DMA((6,)),
    gm_s=DMA((3,)), gm_r=DMA((3,)), gx_s=DMA((3,)), gx_r=DMA((3,)),
    a_s=DMA((4, 2, 3)), a_r=DMA((4, 2, 3)), b_s=DMA((4, 2, 7)), b_r=DMA((4, 2, 7)),
    c_s=DMA((4, 2, 7)), c_r=DMA((4, 2, 7)), d_s=DMA((4, 2, 3)), d_r=DMA((4, 2, 3)),
    e_s=DMA((3, 2)), e_r=DMA((3, 2)),
    q=pltpu.VMEM((2048, 256), BF16), k=pltpu.VMEM((2048, 256), BF16),
    v=pltpu.VMEM((2048, 512), BF16), g=pltpu.VMEM((2048, 512), BF16),
    W=pltpu.VMEM((4, 512, 2048), BF16), R=pltpu.VMEM((3, 512, 512), BF16),
    inner=pltpu.VMEM((2048, 512), F32), prev=pltpu.VMEM((32, DK, DV), BF16),
    a=pltpu.VMEM((32, BLOCK), F32), cum=pltpu.VMEM((32, BLOCK), F32), e=pltpu.VMEM((32, BLOCK), F32),
    fac=pltpu.VMEM((32, BLOCK), F32), run=pltpu.VMEM((2, DK, DV), F32),
    tot_S=pltpu.VMEM((2, DK, DV), F32), tot_f=pltpu.VMEM((2, 1, DV), F32),
    bef_S=pltpu.VMEM((2, DK, DV), F32), bef_f=pltpu.VMEM((2, 1, DV), F32),
    pay=pltpu.VMEM((3, 2, PAY, DV), BF16), got_c=pltpu.VMEM((1, 2, PAY, DV), BF16),
    got_y=pltpu.VMEM((3, 2, PAY, DV), BF16), got_z=pltpu.VMEM((3, 2, PAY, DV), BF16),
    in_sem=DMA((5,)), wx_s=DMA((6,)), wx_r=DMA((6,)), wd_s=DMA((3,)), wd_r=DMA((3,)),
    w1_s=DMA((6,)), w1_r=DMA((6,)), w2_s=DMA((6,)), w2_r=DMA((6,)), w3_s=DMA, w3_r=DMA,
    pre_s=DMA((7,)), pre_r=DMA((7,)), ret_s=DMA((3,)), ret_r=DMA((3,)),
)


def layer_kernel(
    q, k, v, g, ld, wo, x_ref, gain_ref, meta_ref, wg, wu, wd, sg, su, sd, mix_ref, moe_ref, *scratch
):
    ctx = Ctx()
    s = Names()
    for name, ref in zip(SCRATCH, scratch):
        setattr(s, name, ref)
    greet(ctx)
    a = Names()
    m = Names()
    a.__dict__.update(moe_steps(ctx, x_ref, gain_ref, meta_ref, wg, wu, wd, sg, su, sd, moe_ref, s))
    m.__dict__.update(mixer_steps(ctx, q, k, v, g, ld, wo, mix_ref, s))
    m.fetch()
    a.build(0)
    m.spread_x()
    m.decays()
    m.summary()
    m.publish("ep_2")
    a.shared()
    m.inside(0, 2)
    m.absorb("ep_2")
    m.publish("ep_1")
    a.relay(0)
    a.build(1)
    a.build(3)
    m.spread_1()
    m.inside(2, 5)
    m.absorb("ep_1")
    m.publish("ep_0")
    a.relay(1)
    a.relay(3)
    a.weights()
    a.expert(0)
    m.inside(5, 8)
    a.build(2)
    a.expert(1)
    a.give_back(1)
    m.inside(8, 12)
    m.spread_2()
    a.expert(3)
    a.give_back(3)
    a.relay(2)
    m.inside(12, 16)
    m.absorb("ep_0")
    m.gate_in()
    a.relay_back(1)
    m.outer(1)
    a.expert(2)
    a.give_back(2)
    m.outer(3)
    a.relay_back(3)
    a.give_back(0)
    m.outer(2)
    a.fold(1)
    m.outer(0)
    m.spread_3()
    a.relay_back(2)
    a.fold(3)
    a.relay_back(0)
    a.fold(2)
    m.ready()
    m.project(0, 4)
    a.fold(0)
    a.finish()
    m.finish()


def local(
    query_rows, key_rows, value_rows, gate_rows, log_decay, out_proj,
    moe_input, norm_gain, routing, route_weight,
    expert_gate, expert_up, expert_down, shared_gate, shared_up, shared_down,
):
    meta = jnp.concatenate([routing.T.astype(F32), route_weight.T], axis=0)
    vm = pl.BlockSpec(memory_space=pltpu.VMEM)
    hbm = pl.BlockSpec(memory_space=pl.ANY)
    return pl.pallas_call(
        layer_kernel,
        name="layer",
        out_shape=(jax.ShapeDtypeStruct((512, 2048), BF16), jax.ShapeDtypeStruct((N_TOK, 2048), BF16)),
        in_specs=[hbm] * 4 + [vm, hbm] + [vm] * 3 + [hbm] * 6,
        out_specs=(vm, vm),
        scratch_shapes=list(SCRATCH.values()),
        compiler_params=pltpu.CompilerParams(
            collective_id=0, has_side_effects=True, vmem_limit_bytes=67043328
        ),
    )(
        query_rows, key_rows, value_rows, gate_rows, log_decay, out_proj,
        moe_input, norm_gain.reshape(1, -1), meta,
        expert_gate, expert_up, expert_down, shared_gate, shared_up, shared_down,
    )


def solution(mesh):
    split = Mesh(mesh.devices.reshape(4, 4, 2, mesh.shape["tp"]), ("ep_0", "ep_1", "ep_2", "tp"))
    return jax.shard_map(
        local,
        mesh=split,
        in_specs=(
            P(EP, "tp"),
            P(EP, "tp"),
            P(EP, "tp"),
            P(EP, "tp"),
            P("tp", EP),
            P("tp", None),
            P(EP_TP, None),
            P(),
            P(EP_TP, None),
            P(EP_TP, None),
            P(EP_TP, None, None),
            P(EP_TP, None, None),
            P(EP_TP, None, None),
            P(),
            P(),
            P(),
        ),
        out_specs=(P(EP_TP, None), P(EP_TP, None)),
        check_vma=False,
    )
```

```python
import functools

import jax
import jax.numpy as jnp
from jax import lax
from jax.experimental import pallas as pl
from jax.experimental.pallas import tpu as pltpu
from jax.sharding import Mesh
from jax.sharding import PartitionSpec as P

DK = 128
DV = 256
BLOCK = 128
EP = ("ep_0", "ep_1", "ep_2")
EP_TP = ("ep_0", "ep_1", "ep_2", "tp")
EPS = 1e-06
MESH = pl.DeviceIdType.MESH
HI = lax.Precision.HIGHEST
F32 = jnp.float32
BF16 = jnp.bfloat16
SCALE = DK ** (-0.5)

NT = (((1,), (1,)), ((), ()))
TN = (((0,), (0,)), ((), ()))


def dot(a, b, dims=None, precision=None):
    if dims is None:
        dims = (((1,), (0,)), ((), ()))
    return lax.dot_general(a, b, dims, precision=precision, preferred_element_type=F32)


def iota(shape, dim):
    return lax.broadcasted_iota(jnp.int32, shape, dim)


def silu(v):
    half = 0.5 * v
    return half * jnp.tanh(half) + half


N_BLK = 16
HEADS = 2
PAY = DK + 16


def mixer_steps(ctx, q_hbm, k_hbm, v_hbm, g_hbm, ld_ref, wo_ref, out_ref, s):
    z, y, c, x = ctx.z, ctx.y, ctx.c, ctx.x
    start, copy, mod = ctx.start, ctx.copy, ctx.mod
    nb = HEADS * N_BLK

    def rows(first, n):
        return pl.ds(pl.multiple_of(first, 16), n)

    whole = pl.ds(0, 2048)
    direct, half0, half1 = pl.ds(0, 1536), pl.ds(1536, 256), pl.ds(1792, 256)
    r0 = c * 256 + y * 64 + z * 16
    r1 = c * 256 + z * 64 + y * 16
    loads = {}

    def fetch():
        for i, (name, src, dst) in enumerate(
            (("k", k_hbm, s.k), ("v", v_hbm, s.v), ("q", q_hbm, s.q), ("g", g_hbm, s.g), ("w", wo_ref, s.W.at[0]))
        ):
            loads[name] = pltpu.make_async_copy(src, dst, s.in_sem.at[i])
            loads[name].start()

    wx, wd = [], []

    def spread_x():
        for d in (1, 3, 2):
            for h, (r, cols) in enumerate(((r0, half0), (r1, half1))):
                i = (d - 1) * 2 + h
                wx.append(
                    start(wo_ref.at[rows(r, 16), cols], s.W.at[4 - d, rows(r, 16), cols], s.wx_s.at[i], s.wx_r.at[i], tp=d)
                )

    def spread_d():
        for d in (1, 3, 2):
            r = rows(c * 256, 256)
            wd.append(start(wo_ref.at[r, direct], s.W.at[4 - d, r, direct], s.wd_s.at[d - 1], s.wd_r.at[d - 1], tp=d))

    def decays():
        for h in range(HEADS):
            for j in range(N_BLK):
                s.a[h * N_BLK + j : h * N_BLK + j + 1, :] = ld_ref[h : h + 1, j * BLOCK : (j + 1) * BLOCK]
        upper = (iota((BLOCK, BLOCK), 0) <= iota((BLOCK, BLOCK), 1)).astype(F32)
        cum = dot(s.a[...], upper, precision=HI)
        s.cum[...] = cum
        totb = jnp.broadcast_to(cum[:, BLOCK - 1 : BLOCK], (nb, BLOCK))
        ri, ci = iota((nb, nb), 0), iota((nb, nb), 1)
        same = (ri // N_BLK) == (ci // N_BLK)
        after = dot((same & (ci > ri)).astype(F32), totb, precision=HI)
        ahead = dot((same & (ci < ri)).astype(F32), totb, precision=HI)
        s.e[...] = jnp.exp(after + totb - cum) * SCALE
        s.fac[...] = jnp.exp(ahead)
        full = jnp.exp(after + totb)
        s.run[...] = jnp.zeros_like(s.run)
        for h in range(HEADS):
            f = full[h * N_BLK : h * N_BLK + 1, :]
            s.tot_f[h] = jnp.concatenate([f, f], axis=1)

    def col(row):
        return jnp.broadcast_to(row, (BLOCK, BLOCK)).T

    def block(j):
        return pl.ds(pl.multiple_of(j * BLOCK, BLOCK), BLOCK)

    def summary():
        loads["k"].wait()
        loads["v"].wait()

        def body(b, _):
            sl = pl.ds(pl.multiple_of(b * 512, 512), 512)
            for h in range(HEADS):
                scale = jnp.concatenate([col(s.e[pl.ds(h * N_BLK + b * 4 + i, 1), :]) for i in range(4)], axis=0)
                kd = (s.k[sl, h * DK : (h + 1) * DK].astype(F32) * scale).astype(BF16)
                s.run[h] += dot(kd, s.v[sl, h * DV : (h + 1) * DV], TN)
            return 0

        lax.fori_loop(0, 4, body, 0)
        for h in range(HEADS):
            s.tot_S[h] = s.run[h]
        s.run[...] = jnp.zeros_like(s.run)
        loads["q"].wait()

    states = {"ep_2": (s.got_c, 0), "ep_1": (s.got_y, 1), "ep_0": (s.got_z, 4)}
    flying = {}

    def payload(S, f):
        f1 = f.astype(BF16)
        f2 = (f - f1.astype(F32)).astype(BF16)
        row = iota((16, DV), 0)
        top = jnp.where(row == 0, f1.astype(F32), jnp.where(row == 1, f2.astype(F32), 0.0))
        return S.astype(BF16), top.astype(BF16)

    def publish(axis):
        got, base = states[axis]
        if axis == "ep_2":
            src = s.pay_c
            for h in range(HEADS):
                src[h, 0:DK, :], src[h, DK:PAY, :] = payload(s.tot_S[h], s.tot_f[h])
        else:
            src = s.pay.at[base // 4]
            src[0:DK, :], src[DK:PAY, :] = payload(s.tot_S[c], s.tot_f[c])
        flying[axis] = [
            start(src, got.at[d - 1], s.pre_s.at[base + d - 1], s.pre_r.at[base + d - 1], **{axis: d})
            for d in range(1, ctx.size[axis])
        ]

    def scan_over(axis, pieces, own_S, own_f):
        n, at = ctx.size[axis], ctx.place[axis]
        sub_f = jnp.ones((1, DV), F32)
        sub_S = jnp.zeros((DK, DV), F32)
        in_f, in_S = sub_f, sub_S
        for kk in range(n):
            own = at == kk
            slot = jnp.maximum(lax.rem(at - kk + n, n) - 1, 0)
            piece = pieces(slot).astype(F32)
            pf = piece[DK : DK + 1, :] + piece[DK + 1 : DK + 2, :]
            pf = jnp.where(own, own_f, pf)
            ps = jnp.where(own, own_S, piece[0:DK, :])
            if kk:
                in_f = jnp.where(own, sub_f, in_f)
                in_S = jnp.where(own, sub_S, in_S)
            sub_S = pf * sub_S + ps
            sub_f = sub_f * pf
        return in_f, in_S, sub_f, sub_S

    def absorb(axis):
        got, _ = states[axis]
        for cp in flying[axis]:
            cp.wait_recv()
        if axis == "ep_2":
            for h in range(HEADS):
                s.bef_f[h], s.bef_S[h], s.tot_f[h], s.tot_S[h] = scan_over(
                    axis, lambda slot: got[slot, h], s.tot_S[h], s.tot_f[h]
                )
            return
        in_f, in_S, all_f, all_S = scan_over(axis, lambda slot: got[slot], s.tot_S[c], s.tot_f[c])
        if axis == "ep_1":
            s.chip_f[...] = in_f
            s.chip_S[...] = in_S
            s.tot_f[c] = all_f
            s.tot_S[c] = all_S
        else:
            s.chip_S[...] = s.chip_f[...] * in_S + s.chip_S[...]

    def swap():
        flying["end"] = [start(s.chip_S, s.got_e, s.end_s, s.end_r, ep_2=1)]

    def settle():
        for cp in flying["end"]:
            cp.wait_recv()
        for h in range(HEADS):
            before = jnp.where(c == h, s.chip_S[...], s.got_e[...])
            s.bef_S[h] = s.bef_f[h] * before + s.bef_S[h]

    def inside(lo, hi):
        causal = iota((BLOCK, BLOCK), 0) >= iota((BLOCK, BLOCK), 1)

        def body(j, _):
            sl = block(j)
            for h in range(HEADS):
                qb = s.q[sl, h * DK : (h + 1) * DK]
                kb = s.k[sl, h * DK : (h + 1) * DK]
                vb = s.v[sl, h * DV : (h + 1) * DV]
                crow = s.cum[pl.ds(h * N_BLK + j, 1), :]
                ccol = col(crow)
                gap = ccol - jnp.broadcast_to(crow, (BLOCK, BLOCK))
                dec = jnp.exp(jnp.where(causal, gap, -1e30)) * SCALE
                w = (dot(qb, kb, NT) * dec).astype(BF16)
                s.inner[sl, h * DV : (h + 1) * DV] = dot(w, vb)
                last = crow[:, BLOCK - 1 : BLOCK]
                kd = (kb.astype(F32) * (jnp.exp(last - ccol) * SCALE)).astype(BF16)
                s.prev[h * N_BLK + j] = s.run[h].astype(BF16)
                s.run[h] = s.run[h] * jnp.exp(last) + dot(kd, vb, TN)
            return 0

        lax.fori_loop(lo, hi, body, 0)

    def near(axis, d, r, n, cols, ss, rs):
        ref = s.W.at[1:4, rows(r, n), cols]
        return copy(ref, ref, ss, rs, **{axis: d})

    def ring(n, plan, ss, rs, out, into):
        for d in (1, 3, 2):
            for h, (axis, mine, theirs, cols) in enumerate(plan):
                i = (d - 1) * 2 + h
                cp = near(axis, d, mine, n, cols, ss.at[i], rs.at[i])
                cp.start()
                out.append(cp)
                into.append(near(axis, d, theirs(d), n, cols, ss.at[i], rs.at[i]))

    first, first_in, second, second_in, third = [], [], [], [], []

    def spread_1():
        for cp in wx:
            cp.wait_recv()
        ring(
            16,
            (
                ("ep_0", r0, lambda d: c * 256 + y * 64 + mod(z + 4 - d) * 16, half0),
                ("ep_1", r1, lambda d: c * 256 + z * 64 + mod(y + 4 - d) * 16, half1),
            ),
            s.w1_s, s.w1_r, first, first_in,
        )

    def spread_2():
        for cp in first_in:
            cp.wait_recv()
        ring(
            64,
            (
                ("ep_1", c * 256 + y * 64, lambda d: c * 256 + mod(y + 4 - d) * 64, half0),
                ("ep_0", c * 256 + z * 64, lambda d: c * 256 + mod(z + 4 - d) * 64, half1),
            ),
            s.w2_s, s.w2_r, second, second_in,
        )

    def spread_3():
        for cp in second_in + wd:
            cp.wait_recv()
        cp = near("ep_2", 1, c * 256, 256, whole, s.w3_s, s.w3_r)
        cp.start()
        third.extend([cp, near("ep_2", 1, (1 - c) * 256, 256, whole, s.w3_s, s.w3_r)])

    sends = {}

    def outer(d):
        p = mod(x + d)

        def body(i, _):
            j = p * 4 + i
            sl = block(j)
            for h in range(HEADS):
                qb = s.q[sl, h * DK : (h + 1) * DK]
                crow = s.cum[pl.ds(h * N_BLK + j, 1), :]
                grow = jnp.exp(col(crow))
                grow = jnp.concatenate([grow, grow], axis=1)
                fac = s.fac[pl.ds(h * N_BLK + j, 1), :]
                fac = jnp.concatenate([fac, fac], axis=1)
                state = s.prev[h * N_BLK + j].astype(F32) + s.bef_S[h] * fac
                cross = dot(qb, state.astype(BF16))
                raw = s.inner[sl, h * DV : (h + 1) * DV] + cross * grow
                dev = raw - jnp.mean(raw, axis=-1, keepdims=True)
                n = dev * lax.rsqrt(jnp.mean(dev * dev, axis=-1, keepdims=True) + EPS)
                gate = silu(s.g[sl, h * DV : (h + 1) * DV].astype(F32))
                s.g[sl, h * DV : (h + 1) * DV] = (gate * n).astype(BF16)
            return 0

        lax.fori_loop(0, 4, body, 0)
        if d:
            sends[d] = start(
                s.g.at[rows(p * 512, 512), :], s.R.at[3 - d], s.ret_s.at[d - 1], s.ret_r.at[d - 1], tp=d
            )

    def ready():
        loads["w"].wait()
        for cp in sends.values():
            cp.wait_recv()
        third[1].wait_recv()

    def project(lo, hi):
        def body(t, _):
            cols = pl.ds(pl.multiple_of(t * 512, 512), 512)
            acc = dot(s.g[rows(x * 512, 512), :], s.W[0, :, cols])
            for g in (1, 2, 3):
                acc += dot(s.R[g - 1], s.W[g, :, cols])
            s.mix[:, cols] = acc.astype(BF16)
            pltpu.make_async_copy(s.mix.at[:, cols], out_ref.at[:, cols], s.out_sem.at[t]).start()
            return 0

        lax.fori_loop(lo, hi, body, 0)

    def finish():
        for cp in wx + wd + first + second + third[:1] + list(sends.values()) + sum(flying.values(), []):
            cp.wait_send()

    def drain():
        for t in range(4):
            cols = pl.ds(t * 512, 512)
            pltpu.make_async_copy(s.mix.at[:, cols], out_ref.at[:, cols], s.out_sem.at[t]).wait()

    def gate_in():
        loads["g"].wait()

    return dict(
        fetch=fetch, spread_x=spread_x, decays=decays, summary=summary, publish=publish, absorb=absorb, inside=inside,
        spread_1=spread_1, spread_2=spread_2, spread_3=spread_3, outer=outer, ready=ready, project=project,
        finish=finish, gate_in=gate_in, drain=drain, swap=swap, settle=settle, spread_d=spread_d,
    )


N_TOK = 128
TOP = 4
CAP = 8
N_EP = 32
ROWS = N_EP * CAP
HALF = 1024


def moe_steps(ctx, x_ref, gain_ref, rt_ref, wt_ref, wg_hbm, wu_hbm, wd_hbm, sg_hbm, su_hbm, sd_hbm, out_ref, s):
    z, y, c, x = ctx.z, ctx.y, ctx.c, ctx.x
    start, mod = ctx.start, ctx.mod

    def fetch(first, *sources):
        for i, (src, dst) in enumerate(zip(sources, (s.wg, s.wu, s.wd))):
            cp = pltpu.make_async_copy(src, dst, s.load.at[first + i])
            cp.start()
            loads.append(cp)

    loads = []
    fetch(0, sg_hbm, su_hbm, sd_hbm)

    gathers = {}
    sends = []

    def rows_out():
        v = x_ref[...].astype(F32)
        s.X[0] = (v * lax.rsqrt(jnp.mean(v * v, axis=-1, keepdims=True) + EPS) * gain_ref[...]).astype(BF16)
        s.meta[0, 0:TOP, :] = rt_ref[...].astype(F32)
        s.meta[0, TOP : 2 * TOP, :] = wt_ref[...]
        for d in (1, 3, 2):
            a = start(s.meta.at[0], s.meta.at[4 - d], s.gm_s.at[d - 1], s.gm_r.at[d - 1], tp=d)
            b = start(s.X.at[0], s.X.at[4 - d], s.gx_s.at[d - 1], s.gx_r.at[d - 1], tp=d)
            gathers[4 - d] = (a, b)
            sends.extend([a, b])

    def build(gg):
        if gg:
            for cp in gathers[gg]:
                cp.wait_recv()
        rt = s.meta[gg, 0:TOP, :]
        wt = s.meta[gg, TOP : 2 * TOP, :]
        ident = (iota((N_EP, N_TOK), 0) * 4 + x).astype(F32)
        named = jnp.zeros((N_EP, N_TOK), F32)
        weight = jnp.zeros((N_EP, N_TOK), F32)
        for kk in range(TOP):
            hit = rt[kk : kk + 1, :] == ident
            named = named + jnp.where(hit, 1.0, 0.0)
            weight = weight + jnp.where(hit, wt[kk : kk + 1, :], 0.0)
        named = named.astype(BF16)
        earlier = (iota((N_TOK, N_TOK), 0) < iota((N_TOK, N_TOK), 1)).astype(F32).astype(BF16)
        rank = dot(named, earlier).astype(BF16)
        slot = iota((ROWS, N_EP), 0)
        spread = (slot // CAP == iota((ROWS, N_EP), 1)).astype(F32).astype(BF16)
        at = (iota((ROWS, N_TOK), 0) % CAP).astype(F32)
        live = (dot(spread, named) > 0.5) & (dot(spread, rank) == at)
        hi = weight.astype(BF16)
        lo = (weight - hi.astype(F32)).astype(BF16)
        s.whi[gg] = jnp.where(live, dot(spread, hi), 0.0).astype(BF16)
        s.wlo[gg] = jnp.where(live, dot(spread, lo), 0.0).astype(BF16)
        place = jnp.where(live, 1.0, 0.0).astype(BF16)
        for h in range(2):
            rows = dot(place, s.X[gg, :, h * HALF : (h + 1) * HALF]).astype(BF16)
            s.D[gg, h] = rows.reshape(4, 4, 2, CAP, HALF)
        s.M[gg, 0, z] = s.D[gg, 0, z]
        for zz in range(4):
            s.M[gg, 1, y, zz] = s.D[gg, 1, zz, y]
        for d in (1, 3, 2):
            zp, yp = mod(z + d), mod(y + d)
            first[gg, 0].append(
                start(s.D.at[gg, 0, zp], s.M.at[gg, 0, z], s.a_s.at[gg, 0, d - 1], s.a_r.at[gg, 0, d - 1], ep_0=d)
            )
            first[gg, 1].append(
                start(s.D.at[gg, 1, :, yp], s.M.at[gg, 1, y], s.a_s.at[gg, 1, d - 1], s.a_r.at[gg, 1, d - 1], ep_1=d)
            )

    first = {(gg, h): [] for gg in range(4) for h in range(2)}
    second = {(gg, h): [] for gg in range(4) for h in range(2)}
    third = {(gg, h): [] for gg in range(4) for h in range(2)}
    fourth = {(gg, h): [] for gg in range(4) for h in range(2)}
    hops = [(1, 0), (3, 0), (1, 1), (3, 1), (2, 0), (2, 1), (0, 1)]

    def relay(gg):
        for h in range(2):
            for cp in first[gg, h]:
                cp.wait_recv()
            for i, (d, e) in enumerate(hops):
                zp, yp, cp_ = mod(z + d), mod(y + d), lax.rem(c + e, 2)
                if h == 0:
                    src, dst = s.M.at[gg, 0, :, yp, cp_], s.V.at[gg, 0, :, y, c]
                    to = {"ep_1": d, "ep_2": e}
                else:
                    src, dst = s.M.at[gg, 1, :, zp, cp_], s.V.at[gg, 1, z, :, c]
                    to = {"ep_0": d, "ep_2": e}
                second[gg, h].append(start(src, dst, s.b_s.at[gg, h, i], s.b_r.at[gg, h, i], **to))
            for k in range(4):
                if h == 0:
                    s.V[gg, 0, k, y, c] = s.M[gg, 0, k, y, c]
                else:
                    s.V[gg, 1, z, k, c] = s.M[gg, 1, k, z, c]

    def expert(gg):
        for h in range(2):
            for cp in second[gg, h]:
                cp.wait_recv()
        a = s.V[gg, 0].reshape(ROWS, HALF)
        b = s.V[gg, 1].reshape(ROWS, HALF)
        gate = dot(a, s.wg[0:HALF]) + dot(b, s.wg[HALF:])
        up = dot(a, s.wu[0:HALF]) + dot(b, s.wu[HALF:])
        hidden = (silu(gate) * up).astype(BF16)
        for h in range(2):
            rows = dot(hidden, s.wd[:, h * HALF : (h + 1) * HALF]).astype(BF16)
            s.V[gg, h] = rows.reshape(4, 4, 2, CAP, HALF)

    def give_back(gg):
        for h in range(2):
            for i, (d, e) in enumerate(hops):
                zp, yp, cp_ = mod(z + d), mod(y + d), lax.rem(c + e, 2)
                if h == 0:
                    src, dst = s.V.at[gg, 0, :, yp, cp_], s.N.at[gg, 0, :, y, c]
                    to = {"ep_1": d, "ep_2": e}
                else:
                    src, dst = s.V.at[gg, 1, zp, :, cp_], s.N.at[gg, 1, :, z, c]
                    to = {"ep_0": d, "ep_2": e}
                third[gg, h].append(start(src, dst, s.c_s.at[gg, h, i], s.c_r.at[gg, h, i], **to))
            for k in range(4):
                if h == 0:
                    s.N[gg, 0, k, y, c] = s.V[gg, 0, k, y, c]
                else:
                    s.N[gg, 1, k, z, c] = s.V[gg, 1, z, k, c]

    def relay_back(gg):
        for h in range(2):
            for cp in third[gg, h]:
                cp.wait_recv()
            for d in (1, 3, 2):
                zp, yp = mod(z + d), mod(y + d)
                if h == 0:
                    cp = start(s.N.at[gg, 0, zp], s.B.at[gg, 0, z], s.d_s.at[gg, 0, d - 1], s.d_r.at[gg, 0, d - 1], ep_0=d)
                else:
                    cp = start(s.N.at[gg, 1, yp], s.B.at[gg, 1, :, y], s.d_s.at[gg, 1, d - 1], s.d_r.at[gg, 1, d - 1], ep_1=d)
                fourth[gg, h].append(cp)
            if h == 0:
                s.B[gg, 0, z] = s.N[gg, 0, z]
            else:
                for zz in range(4):
                    s.B[gg, 1, zz, y] = s.N[gg, 1, y, zz]

    reduces = {}

    def fold(gg):
        for h in range(2):
            cols = slice(h * HALF, (h + 1) * HALF)
            for cp in fourth[gg, h]:
                cp.wait_recv()
            back = s.B[gg, h].reshape(ROWS, HALF)
            part = dot(s.whi[gg], back, TN) + dot(s.wlo[gg], back, TN)
            if gg == 0:
                s.acc[:, cols] = s.acc[:, cols] + part
            else:
                s.P[gg - 1, h] = part.astype(BF16)
                reduces[gg, h] = start(
                    s.P.at[gg - 1, h], s.G.at[gg - 1, h], s.e_s.at[gg - 1, h], s.e_r.at[gg - 1, h], tp=gg
                )

    def shared():
        for cp in loads[:3]:
            cp.wait()
        rows = s.X[0]
        hidden = (silu(dot(rows, s.wg[...])) * dot(rows, s.wu[...])).astype(BF16)
        for h in range(2):
            cols = slice(h * HALF, (h + 1) * HALF)
            s.acc[:, cols] = dot(hidden, s.wd[:, cols])
        fetch(3, wg_hbm.at[0], wu_hbm.at[0], wd_hbm.at[0])

    def finish():
        for h in range(2):
            cols = slice(h * HALF, (h + 1) * HALF)
            total = s.acc[:, cols]
            for gg in (1, 2, 3):
                reduces[gg, h].wait_recv()
                total = total + s.G[gg - 1, h].astype(F32)
            s.res[:, cols] = total.astype(BF16)
        out = pltpu.make_async_copy(s.res, out_ref, s.res_sem)
        out.start()
        for group in (first, second, third, fourth):
            for cps in group.values():
                for cp in cps:
                    cp.wait_send()
        for cp in list(reduces.values()) + sends:
            cp.wait_send()
        out.wait()

    def weights():
        for cp in loads[3:]:
            cp.wait()

    return dict(
        rows_out=rows_out, build=build, relay=relay, expert=expert, give_back=give_back, relay_back=relay_back,
        fold=fold, shared=shared, finish=finish, weights=weights,
    )


class Names:
    pass


class Ctx:
    def __init__(self):
        self.z = lax.axis_index("ep_0")
        self.y = lax.axis_index("ep_1")
        self.c = lax.axis_index("ep_2")
        self.x = lax.axis_index("tp")
        self.place = {"ep_0": self.z, "ep_1": self.y, "ep_2": self.c, "tp": self.x}
        self.size = {"ep_0": 4, "ep_1": 4, "ep_2": 2, "tp": 4}

    def mod(self, v):
        return lax.rem(v, 4)

    def peer(self, **offsets):
        return {a: lax.rem(self.place[a] + d, self.size[a]) for a, d in offsets.items() if d}

    def copy(self, src, dst, send, recv, **offsets):
        return pltpu.make_async_remote_copy(
            src_ref=src, dst_ref=dst, send_sem=send, recv_sem=recv,
            device_id=self.peer(**offsets), device_id_type=MESH,
        )

    def start(self, src, dst, send, recv, **offsets):
        cp = self.copy(src, dst, send, recv, **offsets)
        cp.start()
        return cp


def greet(ctx):
    peers = [dict(tp=d) for d in (1, 2, 3)]
    peers += [dict(ep_0=d, ep_2=e) for d in (1, 2, 3) for e in (0, 1)]
    peers += [dict(ep_1=d, ep_2=e) for d in (1, 2, 3) for e in (0, 1)]
    peers += [dict(ep_2=1)]
    barrier = pltpu.get_barrier_semaphore()
    for p in peers:
        pl.semaphore_signal(barrier, inc=1, device_id=ctx.peer(**p), device_id_type=MESH)
    pl.semaphore_wait(barrier, len(peers))


DMA = pltpu.SemaphoreType.DMA
BLK = (4, 4, 2, CAP, HALF)
SCRATCH = dict(
    wg=pltpu.VMEM((2048, 512), BF16), wu=pltpu.VMEM((2048, 512), BF16), wd=pltpu.VMEM((512, 2048), BF16),
    X=pltpu.VMEM((4, N_TOK, 2048), BF16), meta=pltpu.VMEM((4, 8, N_TOK), F32),
    whi=pltpu.VMEM((4, ROWS, N_TOK), BF16), wlo=pltpu.VMEM((4, ROWS, N_TOK), BF16),
    D=pltpu.VMEM((4, 2) + BLK, BF16), M=pltpu.VMEM((4, 2) + BLK, BF16), V=pltpu.VMEM((4, 2) + BLK, BF16),
    N=pltpu.VMEM((4, 2) + BLK, BF16), B=pltpu.VMEM((4, 2) + BLK, BF16),
    acc=pltpu.VMEM((N_TOK, 2048), F32),
    P=pltpu.VMEM((3, 2, N_TOK, HALF), BF16), G=pltpu.VMEM((3, 2, N_TOK, HALF), BF16),
    load=DMA((6,)),
    gm_s=DMA((3,)), gm_r=DMA((3,)), gx_s=DMA((3,)), gx_r=DMA((3,)),
    a_s=DMA((4, 2, 3)), a_r=DMA((4, 2, 3)), b_s=DMA((4, 2, 7)), b_r=DMA((4, 2, 7)),
    c_s=DMA((4, 2, 7)), c_r=DMA((4, 2, 7)), d_s=DMA((4, 2, 3)), d_r=DMA((4, 2, 3)),
    e_s=DMA((3, 2)), e_r=DMA((3, 2)),
    q=pltpu.VMEM((2048, 256), BF16), k=pltpu.VMEM((2048, 256), BF16),
    v=pltpu.VMEM((2048, 512), BF16), g=pltpu.VMEM((2048, 512), BF16),
    W=pltpu.VMEM((4, 512, 2048), BF16), R=pltpu.VMEM((3, 512, 512), BF16),
    inner=pltpu.VMEM((2048, 512), F32), prev=pltpu.VMEM((32, DK, DV), BF16),
    a=pltpu.VMEM((32, BLOCK), F32), cum=pltpu.VMEM((32, BLOCK), F32), e=pltpu.VMEM((32, BLOCK), F32),
    fac=pltpu.VMEM((32, BLOCK), F32), run=pltpu.VMEM((2, DK, DV), F32),
    tot_S=pltpu.VMEM((2, DK, DV), F32), tot_f=pltpu.VMEM((2, 1, DV), F32),
    bef_S=pltpu.VMEM((2, DK, DV), F32), bef_f=pltpu.VMEM((2, 1, DV), F32),
    pay_c=pltpu.VMEM((2, PAY, DV), BF16), pay=pltpu.VMEM((2, PAY, DV), BF16), got_c=pltpu.VMEM((1, 2, PAY, DV), BF16),
    got_y=pltpu.VMEM((3, PAY, DV), BF16), got_z=pltpu.VMEM((3, PAY, DV), BF16),
    chip_S=pltpu.VMEM((DK, DV), F32), chip_f=pltpu.VMEM((1, DV), F32), got_e=pltpu.VMEM((DK, DV), F32),
    end_s=DMA, end_r=DMA,
    mix=pltpu.VMEM((512, 2048), BF16), res=pltpu.VMEM((N_TOK, 2048), BF16), out_sem=DMA((4,)), res_sem=DMA,
    in_sem=DMA((5,)), wx_s=DMA((6,)), wx_r=DMA((6,)), wd_s=DMA((3,)), wd_r=DMA((3,)),
    w1_s=DMA((6,)), w1_r=DMA((6,)), w2_s=DMA((6,)), w2_r=DMA((6,)), w3_s=DMA, w3_r=DMA,
    pre_s=DMA((7,)), pre_r=DMA((7,)), ret_s=DMA((3,)), ret_r=DMA((3,)),
)


def layer_kernel(
    q, k, v, g, ld, wo, x_ref, gain_ref, rt_ref, wt_ref, wg, wu, wd, sg, su, sd, mix_ref, moe_ref, *scratch
):
    ctx = Ctx()
    s = Names()
    for name, ref in zip(SCRATCH, scratch):
        setattr(s, name, ref)
    greet(ctx)
    a = Names()
    m = Names()
    a.__dict__.update(moe_steps(ctx, x_ref, gain_ref, rt_ref, wt_ref, wg, wu, wd, sg, su, sd, moe_ref, s))
    m.__dict__.update(mixer_steps(ctx, q, k, v, g, ld, wo, mix_ref, s))
    m.spread_x()
    m.fetch()
    a.rows_out()
    a.build(0)
    m.spread_d()
    m.decays()
    m.spread_1()
    m.summary()
    m.publish("ep_2")
    a.shared()
    m.spread_2()
    m.absorb("ep_2")
    m.publish("ep_1")
    a.relay(0)
    m.inside(0, 4)
    a.build(1)
    a.build(3)
    m.absorb("ep_1")
    m.publish("ep_0")
    m.inside(4, 8)
    a.weights()
    a.expert(0)
    a.relay(1)
    a.build(2)
    m.inside(8, 12)
    a.relay(3)
    m.absorb("ep_0")
    m.swap()
    m.inside(12, 16)
    m.settle()
    m.gate_in()
    a.expert(1)
    a.relay(2)
    a.give_back(1)
    m.outer(1)
    m.outer(3)
    m.outer(2)
    a.expert(3)
    a.give_back(3)
    m.outer(0)
    a.expert(2)
    a.give_back(2)
    m.spread_3()
    a.relay_back(1)
    a.relay_back(3)
    a.give_back(0)
    a.fold(1)
    a.relay_back(2)
    a.fold(3)
    m.ready()
    m.project(0, 2)
    a.relay_back(0)
    a.fold(2)
    m.project(2, 4)
    a.fold(0)
    a.finish()
    m.finish()
    m.drain()


def local(
    query_rows, key_rows, value_rows, gate_rows, log_decay, out_proj,
    moe_input, norm_gain, routing, route_weight,
    expert_gate, expert_up, expert_down, shared_gate, shared_up, shared_down,
):
    vm = pl.BlockSpec(memory_space=pltpu.VMEM)
    hbm = pl.BlockSpec(memory_space=pl.ANY)
    return pl.pallas_call(
        layer_kernel,
        name="layer",
        out_shape=(jax.ShapeDtypeStruct((512, 2048), BF16), jax.ShapeDtypeStruct((N_TOK, 2048), BF16)),
        in_specs=[hbm] * 4 + [vm, hbm] + [vm] * 4 + [hbm] * 6,
        out_specs=(hbm, hbm),
        scratch_shapes=list(SCRATCH.values()),
        compiler_params=pltpu.CompilerParams(
            collective_id=0, has_side_effects=True, vmem_limit_bytes=67043328
        ),
    )(
        query_rows, key_rows, value_rows, gate_rows, log_decay, out_proj,
        moe_input, norm_gain.reshape(1, -1), routing.T, route_weight.T,
        expert_gate, expert_up, expert_down, shared_gate, shared_up, shared_down,
    )


def solution(mesh):
    split = Mesh(mesh.devices.reshape(4, 4, 2, mesh.shape["tp"]), ("ep_0", "ep_1", "ep_2", "tp"))
    return jax.shard_map(
        local,
        mesh=split,
        in_specs=(
            P(EP, "tp"),
            P(EP, "tp"),
            P(EP, "tp"),
            P(EP, "tp"),
            P("tp", EP),
            P("tp", None),
            P(EP_TP, None),
            P(),
            P(EP_TP, None),
            P(EP_TP, None),
            P(EP_TP, None, None),
            P(EP_TP, None, None),
            P(EP_TP, None, None),
            P(),
            P(),
            P(),
        ),
        out_specs=(P(EP_TP, None), P(EP_TP, None)),
        check_vma=False,
    )
```

```python
import functools

import jax
import jax.numpy as jnp
from jax import lax
from jax.experimental import pallas as pl
from jax.experimental.pallas import tpu as pltpu
from jax.sharding import Mesh
from jax.sharding import PartitionSpec as P

DK = 128
DV = 256
BLOCK = 128
EP = ("ep_0", "ep_1", "ep_2")
EP_TP = ("ep_0", "ep_1", "ep_2", "tp")
EPS = 1e-06
MESH = pl.DeviceIdType.MESH
HI = lax.Precision.HIGHEST
F32 = jnp.float32
BF16 = jnp.bfloat16
SCALE = DK ** (-0.5)

NT = (((1,), (1,)), ((), ()))
TN = (((0,), (0,)), ((), ()))


def dot(a, b, dims=None, precision=None):
    if dims is None:
        dims = (((1,), (0,)), ((), ()))
    return lax.dot_general(a, b, dims, precision=precision, preferred_element_type=F32)


def iota(shape, dim):
    return lax.broadcasted_iota(jnp.int32, shape, dim)


def silu(v):
    half = 0.5 * v
    return half * jnp.tanh(half) + half


N_BLK = 16
HEADS = 2
PAY = DK + 16


def mixer_steps(ctx, q_hbm, k_hbm, v_hbm, g_hbm, ld_ref, wo_ref, out_ref, s):
    z, y, c, x = ctx.z, ctx.y, ctx.c, ctx.x
    start, copy, mod = ctx.start, ctx.copy, ctx.mod
    nb = HEADS * N_BLK

    def rows(first, n):
        return pl.ds(pl.multiple_of(first, 16), n)

    whole, left, right = pl.ds(0, 2048), pl.ds(0, 1024), pl.ds(1024, 1024)
    mine = rows(c * 256, 256)
    loads = {}

    def fetch():
        for i, (name, src, dst) in enumerate(
            (("k", k_hbm, s.k), ("v", v_hbm, s.v), ("q", q_hbm, s.q), ("g", g_hbm, s.g), ("w", wo_ref, s.W.at[0]))
        ):
            loads[name] = pltpu.make_async_copy(src, dst, s.in_sem.at[i])
            loads[name].start()

    wd, wf = {}, []

    def spread_d():
        for d in (1, 3):
            wd[d] = start(wo_ref.at[mine, whole], s.W.at[4 - d, mine, whole], s.wd_s.at[d // 2], s.wd_r.at[d // 2], tp=d)

    def spread_f():
        for d, cols in ((3, left), (1, right)):
            wd[d].wait_recv()
            wf.append(
                start(s.W.at[4 - d, mine, cols], s.W.at[2, mine, cols], s.wf_s.at[d // 2], s.wf_r.at[d // 2], tp=d)
            )

    def decays():
        for h in range(HEADS):
            for j in range(N_BLK):
                s.a[h * N_BLK + j : h * N_BLK + j + 1, :] = ld_ref[h : h + 1, j * BLOCK : (j + 1) * BLOCK]
        upper = (iota((BLOCK, BLOCK), 0) <= iota((BLOCK, BLOCK), 1)).astype(F32)
        cum = dot(s.a[...], upper, precision=HI)
        s.cum[...] = cum
        totb = jnp.broadcast_to(cum[:, BLOCK - 1 : BLOCK], (nb, BLOCK))
        ri, ci = iota((nb, nb), 0), iota((nb, nb), 1)
        same = (ri // N_BLK) == (ci // N_BLK)
        after = dot((same & (ci > ri)).astype(F32), totb, precision=HI)
        ahead = dot((same & (ci < ri)).astype(F32), totb, precision=HI)
        s.e[...] = jnp.exp(after + totb - cum) * SCALE
        s.fac[...] = jnp.exp(ahead)
        full = jnp.exp(after + totb)
        s.run[...] = jnp.zeros_like(s.run)
        for h in range(HEADS):
            f = full[h * N_BLK : h * N_BLK + 1, :]
            s.tot_f[h] = jnp.concatenate([f, f], axis=1)

    def col(row):
        return jnp.broadcast_to(row, (BLOCK, BLOCK)).T

    def block(j):
        return pl.ds(pl.multiple_of(j * BLOCK, BLOCK), BLOCK)

    def summary():
        loads["k"].wait()
        loads["v"].wait()

        def body(b, _):
            sl = pl.ds(pl.multiple_of(b * 512, 512), 512)
            for h in range(HEADS):
                scale = jnp.concatenate([col(s.e[pl.ds(h * N_BLK + b * 4 + i, 1), :]) for i in range(4)], axis=0)
                kd = (s.k[sl, h * DK : (h + 1) * DK].astype(F32) * scale).astype(BF16)
                s.run[h] += dot(kd, s.v[sl, h * DV : (h + 1) * DV], TN)
            return 0

        lax.fori_loop(0, 4, body, 0)
        for h in range(HEADS):
            s.tot_S[h] = s.run[h]
        s.run[...] = jnp.zeros_like(s.run)
        loads["q"].wait()

    states = {"ep_2": (s.got_c, 0), "ep_1": (s.got_y, 1), "ep_0": (s.got_z, 4)}
    flying = {}

    def payload(S, f):
        f1 = f.astype(BF16)
        f2 = (f - f1.astype(F32)).astype(BF16)
        row = iota((16, DV), 0)
        top = jnp.where(row == 0, f1.astype(F32), jnp.where(row == 1, f2.astype(F32), 0.0))
        return S.astype(BF16), top.astype(BF16)

    def publish(axis):
        got, base = states[axis]
        if axis == "ep_2":
            src = s.pay_c
            for h in range(HEADS):
                src[h, 0:DK, :], src[h, DK:PAY, :] = payload(s.tot_S[h], s.tot_f[h])
        else:
            src = s.pay.at[base // 4]
            src[0:DK, :], src[DK:PAY, :] = payload(s.tot_S[c], s.tot_f[c])
        flying[axis] = [
            start(src, got.at[d - 1], s.pre_s.at[base + d - 1], s.pre_r.at[base + d - 1], **{axis: d})
            for d in range(1, ctx.size[axis])
        ]

    def scan_over(axis, pieces, own_S, own_f):
        n, at = ctx.size[axis], ctx.place[axis]
        sub_f = jnp.ones((1, DV), F32)
        sub_S = jnp.zeros((DK, DV), F32)
        in_f, in_S = sub_f, sub_S
        for kk in range(n):
            own = at == kk
            slot = jnp.maximum(lax.rem(at - kk + n, n) - 1, 0)
            piece = pieces(slot).astype(F32)
            pf = piece[DK : DK + 1, :] + piece[DK + 1 : DK + 2, :]
            pf = jnp.where(own, own_f, pf)
            ps = jnp.where(own, own_S, piece[0:DK, :])
            if kk:
                in_f = jnp.where(own, sub_f, in_f)
                in_S = jnp.where(own, sub_S, in_S)
            sub_S = pf * sub_S + ps
            sub_f = sub_f * pf
        return in_f, in_S, sub_f, sub_S

    def absorb(axis):
        got, _ = states[axis]
        for cp in flying[axis]:
            cp.wait_recv()
        if axis == "ep_2":
            for h in range(HEADS):
                s.bef_f[h], s.bef_S[h], s.tot_f[h], s.tot_S[h] = scan_over(
                    axis, lambda slot: got[slot, h], s.tot_S[h], s.tot_f[h]
                )
            return
        in_f, in_S, all_f, all_S = scan_over(axis, lambda slot: got[slot], s.tot_S[c], s.tot_f[c])
        if axis == "ep_1":
            s.chip_f[...] = in_f
            s.chip_S[...] = in_S
            s.tot_f[c] = all_f
            s.tot_S[c] = all_S
        else:
            s.chip_S[...] = s.chip_f[...] * in_S + s.chip_S[...]

    def swap():
        flying["end"] = [start(s.chip_S, s.got_e, s.end_s, s.end_r, ep_2=1)]

    def settle():
        for cp in flying["end"]:
            cp.wait_recv()
        for h in range(HEADS):
            before = jnp.where(c == h, s.chip_S[...], s.got_e[...])
            s.bef_S[h] = s.bef_f[h] * before + s.bef_S[h]

    def inside(lo, hi):
        causal = iota((BLOCK, BLOCK), 0) >= iota((BLOCK, BLOCK), 1)

        def body(j, _):
            sl = block(j)
            for h in range(HEADS):
                qb = s.q[sl, h * DK : (h + 1) * DK]
                kb = s.k[sl, h * DK : (h + 1) * DK]
                vb = s.v[sl, h * DV : (h + 1) * DV]
                crow = s.cum[pl.ds(h * N_BLK + j, 1), :]
                ccol = col(crow)
                gap = ccol - jnp.broadcast_to(crow, (BLOCK, BLOCK))
                dec = jnp.exp(jnp.where(causal, gap, -1e30)) * SCALE
                w = (dot(qb, kb, NT) * dec).astype(BF16)
                s.inner[sl, h * DV : (h + 1) * DV] = dot(w, vb)
                last = crow[:, BLOCK - 1 : BLOCK]
                kd = (kb.astype(F32) * (jnp.exp(last - ccol) * SCALE)).astype(BF16)
                s.prev[h * N_BLK + j] = s.run[h].astype(BF16)
                s.run[h] = s.run[h] * jnp.exp(last) + dot(kd, vb, TN)
            return 0

        lax.fori_loop(lo, hi, body, 0)

    def near(r):
        ref = s.W.at[1:4, rows(r, 256), whole]
        return copy(ref, ref, s.w3_s, s.w3_r, ep_2=1)

    third = []

    def spread_3():
        for cp in wf:
            cp.wait_recv()
        third.extend([near(c * 256), near((1 - c) * 256)])
        third[0].start()

    sends = {}

    def outer(d):
        p = mod(x + d)

        def body(i, _):
            j = p * 4 + i
            sl = block(j)
            for h in range(HEADS):
                qb = s.q[sl, h * DK : (h + 1) * DK]
                crow = s.cum[pl.ds(h * N_BLK + j, 1), :]
                grow = jnp.exp(col(crow))
                grow = jnp.concatenate([grow, grow], axis=1)
                fac = s.fac[pl.ds(h * N_BLK + j, 1), :]
                fac = jnp.concatenate([fac, fac], axis=1)
                state = s.prev[h * N_BLK + j].astype(F32) + s.bef_S[h] * fac
                cross = dot(qb, state.astype(BF16))
                raw = s.inner[sl, h * DV : (h + 1) * DV] + cross * grow
                dev = raw - jnp.mean(raw, axis=-1, keepdims=True)
                n = dev * lax.rsqrt(jnp.mean(dev * dev, axis=-1, keepdims=True) + EPS)
                gate = silu(s.g[sl, h * DV : (h + 1) * DV].astype(F32))
                s.g[sl, h * DV : (h + 1) * DV] = (gate * n).astype(BF16)
            return 0

        lax.fori_loop(0, 4, body, 0)
        if d:
            sends[d] = start(
                s.g.at[rows(p * 512, 512), :], s.R.at[3 - d], s.ret_s.at[d - 1], s.ret_r.at[d - 1], tp=d
            )

    def ready():
        loads["w"].wait()
        for cp in sends.values():
            cp.wait_recv()
        third[1].wait_recv()

    def project(lo, hi):
        def body(t, _):
            cols = pl.ds(pl.multiple_of(t * 512, 512), 512)
            acc = dot(s.g[rows(x * 512, 512), :], s.W[0, :, cols])
            for g in (1, 2, 3):
                acc += dot(s.R[g - 1], s.W[g, :, cols])
            s.mix[:, cols] = acc.astype(BF16)
            pltpu.make_async_copy(s.mix.at[:, cols], out_ref.at[:, cols], s.out_sem.at[t]).start()
            return 0

        lax.fori_loop(lo, hi, body, 0)

    def finish():
        for cp in list(wd.values()) + wf + third[:1] + list(sends.values()) + sum(flying.values(), []):
            cp.wait_send()

    def drain():
        for t in range(4):
            cols = pl.ds(t * 512, 512)
            pltpu.make_async_copy(s.mix.at[:, cols], out_ref.at[:, cols], s.out_sem.at[t]).wait()

    def gate_in():
        loads["g"].wait()

    return dict(
        fetch=fetch, decays=decays, summary=summary, publish=publish, absorb=absorb, inside=inside,
        spread_3=spread_3, spread_f=spread_f, outer=outer, ready=ready, project=project,
        finish=finish, gate_in=gate_in, drain=drain, swap=swap, settle=settle, spread_d=spread_d,
    )


N_TOK = 128
TOP = 4
CAP = 8
N_EP = 32
ROWS = N_EP * CAP
HALF = 1024


def moe_steps(ctx, x_ref, gain_ref, rt_ref, wt_ref, wg_hbm, wu_hbm, wd_hbm, sg_hbm, su_hbm, sd_hbm, out_ref, s):
    z, y, c, x = ctx.z, ctx.y, ctx.c, ctx.x
    start, mod = ctx.start, ctx.mod

    def fetch(first, *sources):
        for i, (src, dst) in enumerate(zip(sources, (s.wg, s.wu, s.wd))):
            cp = pltpu.make_async_copy(src, dst, s.load.at[first + i])
            cp.start()
            loads.append(cp)

    loads = []
    fetch(0, sg_hbm, su_hbm, sd_hbm)

    gathers = {}
    sends = []

    def rows_out():
        v = x_ref[...].astype(F32)
        s.X[0] = (v * lax.rsqrt(jnp.mean(v * v, axis=-1, keepdims=True) + EPS) * gain_ref[...]).astype(BF16)
        s.meta[0, 0:TOP, :] = rt_ref[...].astype(F32)
        s.meta[0, TOP : 2 * TOP, :] = wt_ref[...]
        for d in (1, 3, 2):
            sends.append(start(s.meta.at[0], s.meta.at[4 - d], s.gm_s.at[d - 1], s.gm_r.at[d - 1], tp=d))
            gathers[4 - d] = [sends[-1]]
        for d in (1, 3):
            sends.append(start(s.X.at[0], s.X.at[4 - d], s.gx_s.at[d // 2], s.gx_r.at[d // 2], tp=d))
            gathers[4 - d].append(sends[-1])

    def group(ss, rs, gg, h, n):
        ref = s.W.at[0, 0:n, :]
        return ctx.copy(ref, ref, ss.at[gg, h], rs.at[gg, h], tp=1)

    def build(gg):
        if gg:
            for cp in gathers[gg]:
                cp.wait_recv()
            if gg != 2:
                part = pl.ds((gg // 2) * HALF, HALF)
                sends.append(
                    start(s.X.at[gg, :, part], s.X.at[2, :, part], s.gf_s.at[gg // 2], s.gf_r.at[gg // 2], tp=4 - gg)
                )
                gathers[2].append(sends[-1])
        rt = s.meta[gg, 0:TOP, :]
        wt = s.meta[gg, TOP : 2 * TOP, :]
        ident = (iota((N_EP, N_TOK), 0) * 4 + x).astype(F32)
        named = jnp.zeros((N_EP, N_TOK), F32)
        weight = jnp.zeros((N_EP, N_TOK), F32)
        for kk in range(TOP):
            hit = rt[kk : kk + 1, :] == ident
            named = named + jnp.where(hit, 1.0, 0.0)
            weight = weight + jnp.where(hit, wt[kk : kk + 1, :], 0.0)
        named = named.astype(BF16)
        earlier = (iota((N_TOK, N_TOK), 0) < iota((N_TOK, N_TOK), 1)).astype(F32).astype(BF16)
        rank = dot(named, earlier).astype(BF16)
        slot = iota((ROWS, N_EP), 0)
        spread = (slot // CAP == iota((ROWS, N_EP), 1)).astype(F32).astype(BF16)
        at = (iota((ROWS, N_TOK), 0) % CAP).astype(F32)
        live = (dot(spread, named) > 0.5) & (dot(spread, rank) == at)
        hi = weight.astype(BF16)
        lo = (weight - hi.astype(F32)).astype(BF16)
        s.whi[gg] = jnp.where(live, dot(spread, hi), 0.0).astype(BF16)
        s.wlo[gg] = jnp.where(live, dot(spread, lo), 0.0).astype(BF16)
        place = jnp.where(live, 1.0, 0.0).astype(BF16)
        for h in range(2):
            rows = dot(place, s.X[gg, :, h * HALF : (h + 1) * HALF]).astype(BF16)
            s.D[gg, h] = rows.reshape(4, 4, 2, CAP, HALF)
        s.M[gg, 0, z] = s.D[gg, 0, z]
        for zz in range(4):
            s.M[gg, 1, y, zz] = s.D[gg, 1, zz, y]
        for d in (1, 3, 2):
            zp, yp = mod(z + d), mod(y + d)
            start(s.D.at[gg, 0, zp], s.M.at[gg, 0, z], s.a_s.at[gg, 0], s.a_r.at[gg, 0], ep_0=d)
            start(s.D.at[gg, 1, :, yp], s.M.at[gg, 1, y], s.a_s.at[gg, 1], s.a_r.at[gg, 1], ep_1=d)

    hops = [(1, 0), (3, 0), (1, 1), (3, 1), (2, 0), (2, 1), (0, 1)]

    def relay(gg):
        for h in range(2):
            group(s.a_s, s.a_r, gg, h, 96).wait_recv()
            for i, (d, e) in enumerate(hops):
                zp, yp, cp_ = mod(z + d), mod(y + d), lax.rem(c + e, 2)
                if h == 0:
                    src, dst = s.M.at[gg, 0, :, yp, cp_], s.V.at[gg, 0, :, y, c]
                    to = {"ep_1": d, "ep_2": e}
                else:
                    src, dst = s.M.at[gg, 1, :, zp, cp_], s.V.at[gg, 1, z, :, c]
                    to = {"ep_0": d, "ep_2": e}
                start(src, dst, s.b_s.at[gg, h], s.b_r.at[gg, h], **to)
            for k in range(4):
                if h == 0:
                    s.V[gg, 0, k, y, c] = s.M[gg, 0, k, y, c]
                else:
                    s.V[gg, 1, z, k, c] = s.M[gg, 1, k, z, c]

    def expert(gg):
        for h in range(2):
            group(s.b_s, s.b_r, gg, h, 112).wait_recv()
        a = s.V[gg, 0].reshape(ROWS, HALF)
        b = s.V[gg, 1].reshape(ROWS, HALF)
        gate = dot(a, s.wg[0:HALF]) + dot(b, s.wg[HALF:])
        up = dot(a, s.wu[0:HALF]) + dot(b, s.wu[HALF:])
        hidden = (silu(gate) * up).astype(BF16)
        for h in range(2):
            rows = dot(hidden, s.wd[:, h * HALF : (h + 1) * HALF]).astype(BF16)
            s.V[gg, h] = rows.reshape(4, 4, 2, CAP, HALF)

    def give_back(gg):
        for h in range(2):
            for i, (d, e) in enumerate(hops):
                zp, yp, cp_ = mod(z + d), mod(y + d), lax.rem(c + e, 2)
                if h == 0:
                    src, dst = s.V.at[gg, 0, :, yp, cp_], s.N.at[gg, 0, :, y, c]
                    to = {"ep_1": d, "ep_2": e}
                else:
                    src, dst = s.V.at[gg, 1, zp, :, cp_], s.N.at[gg, 1, :, z, c]
                    to = {"ep_0": d, "ep_2": e}
                start(src, dst, s.c_s.at[gg, h], s.c_r.at[gg, h], **to)
            for k in range(4):
                if h == 0:
                    s.N[gg, 0, k, y, c] = s.V[gg, 0, k, y, c]
                else:
                    s.N[gg, 1, k, z, c] = s.V[gg, 1, z, k, c]

    def relay_back(gg):
        for h in range(2):
            group(s.c_s, s.c_r, gg, h, 112).wait_recv()
            for d in (1, 3, 2):
                zp, yp = mod(z + d), mod(y + d)
                if h == 0:
                    start(s.N.at[gg, 0, zp], s.B.at[gg, 0, z], s.d_s.at[gg, 0], s.d_r.at[gg, 0], ep_0=d)
                else:
                    start(s.N.at[gg, 1, yp], s.B.at[gg, 1, :, y], s.d_s.at[gg, 1], s.d_r.at[gg, 1], ep_1=d)
            if h == 0:
                s.B[gg, 0, z] = s.N[gg, 0, z]
            else:
                for zz in range(4):
                    s.B[gg, 1, zz, y] = s.N[gg, 1, y, zz]

    reduces = {}

    def fold(gg):
        for h in range(2):
            cols = slice(h * HALF, (h + 1) * HALF)
            group(s.d_s, s.d_r, gg, h, 96).wait_recv()
            back = s.B[gg, h].reshape(ROWS, HALF)
            part = dot(s.whi[gg], back, TN) + dot(s.wlo[gg], back, TN)
            if gg == 0:
                s.acc[:, cols] = s.acc[:, cols] + part
            else:
                s.P[gg - 1, h] = part.astype(BF16)
                reduces[gg, h] = start(
                    s.P.at[gg - 1, h], s.G.at[gg - 1, h], s.e_s.at[gg - 1, h], s.e_r.at[gg - 1, h], tp=gg
                )

    def shared():
        for cp in loads[:3]:
            cp.wait()
        rows = s.X[0]
        hidden = (silu(dot(rows, s.wg[...])) * dot(rows, s.wu[...])).astype(BF16)
        for h in range(2):
            cols = slice(h * HALF, (h + 1) * HALF)
            s.acc[:, cols] = dot(hidden, s.wd[:, cols])
        fetch(3, wg_hbm.at[0], wu_hbm.at[0], wd_hbm.at[0])

    def finish():
        for h in range(2):
            cols = slice(h * HALF, (h + 1) * HALF)
            total = s.acc[:, cols]
            for gg in (1, 2, 3):
                reduces[gg, h].wait_recv()
                total = total + s.G[gg - 1, h].astype(F32)
            s.res[:, cols] = total.astype(BF16)
        out = pltpu.make_async_copy(s.res, out_ref, s.res_sem)
        out.start()
        for gg in range(4):
            for h in range(2):
                for ss, rs, n in ((s.a_s, s.a_r, 96), (s.b_s, s.b_r, 112), (s.c_s, s.c_r, 112), (s.d_s, s.d_r, 96)):
                    group(ss, rs, gg, h, n).wait_send()
        for cp in list(reduces.values()) + sends:
            cp.wait_send()
        out.wait()

    def weights():
        for cp in loads[3:]:
            cp.wait()

    return dict(
        rows_out=rows_out, build=build, relay=relay, expert=expert, give_back=give_back, relay_back=relay_back,
        fold=fold, shared=shared, finish=finish, weights=weights,
    )


class Names:
    pass


class Ctx:
    def __init__(self):
        self.z = lax.axis_index("ep_0")
        self.y = lax.axis_index("ep_1")
        self.c = lax.axis_index("ep_2")
        self.x = lax.axis_index("tp")
        self.place = {"ep_0": self.z, "ep_1": self.y, "ep_2": self.c, "tp": self.x}
        self.size = {"ep_0": 4, "ep_1": 4, "ep_2": 2, "tp": 4}

    def mod(self, v):
        return lax.rem(v, 4)

    def peer(self, **offsets):
        return {a: lax.rem(self.place[a] + d, self.size[a]) for a, d in offsets.items() if d}

    def copy(self, src, dst, send, recv, **offsets):
        return pltpu.make_async_remote_copy(
            src_ref=src, dst_ref=dst, send_sem=send, recv_sem=recv,
            device_id=self.peer(**offsets), device_id_type=MESH,
        )

    def start(self, src, dst, send, recv, **offsets):
        cp = self.copy(src, dst, send, recv, **offsets)
        cp.start()
        return cp


def greet(ctx):
    peers = [dict(tp=d) for d in (1, 2, 3)]
    peers += [dict(ep_0=d, ep_2=e) for d in (1, 2, 3) for e in (0, 1)]
    peers += [dict(ep_1=d, ep_2=e) for d in (1, 2, 3) for e in (0, 1)]
    peers += [dict(ep_2=1)]
    barrier = pltpu.get_barrier_semaphore()
    for p in peers:
        pl.semaphore_signal(barrier, inc=1, device_id=ctx.peer(**p), device_id_type=MESH)
    pl.semaphore_wait(barrier, len(peers))


DMA = pltpu.SemaphoreType.DMA
BLK = (4, 4, 2, CAP, HALF)
SCRATCH = dict(
    wg=pltpu.VMEM((2048, 512), BF16), wu=pltpu.VMEM((2048, 512), BF16), wd=pltpu.VMEM((512, 2048), BF16),
    X=pltpu.VMEM((4, N_TOK, 2048), BF16), meta=pltpu.VMEM((4, 8, N_TOK), F32),
    whi=pltpu.VMEM((4, ROWS, N_TOK), BF16), wlo=pltpu.VMEM((4, ROWS, N_TOK), BF16),
    D=pltpu.VMEM((4, 2) + BLK, BF16), M=pltpu.VMEM((4, 2) + BLK, BF16), V=pltpu.VMEM((4, 2) + BLK, BF16),
    N=pltpu.VMEM((4, 2) + BLK, BF16), B=pltpu.VMEM((4, 2) + BLK, BF16),
    acc=pltpu.VMEM((N_TOK, 2048), F32),
    P=pltpu.VMEM((3, 2, N_TOK, HALF), BF16), G=pltpu.VMEM((3, 2, N_TOK, HALF), BF16),
    load=DMA((6,)),
    gm_s=DMA((3,)), gm_r=DMA((3,)), gx_s=DMA((2,)), gx_r=DMA((2,)), gf_s=DMA((2,)), gf_r=DMA((2,)),
    a_s=DMA((4, 2)), a_r=DMA((4, 2)), b_s=DMA((4, 2)), b_r=DMA((4, 2)),
    c_s=DMA((4, 2)), c_r=DMA((4, 2)), d_s=DMA((4, 2)), d_r=DMA((4, 2)),
    e_s=DMA((3, 2)), e_r=DMA((3, 2)),
    q=pltpu.VMEM((2048, 256), BF16), k=pltpu.VMEM((2048, 256), BF16),
    v=pltpu.VMEM((2048, 512), BF16), g=pltpu.VMEM((2048, 512), BF16),
    W=pltpu.VMEM((4, 512, 2048), BF16), R=pltpu.VMEM((3, 512, 512), BF16),
    inner=pltpu.VMEM((2048, 512), F32), prev=pltpu.VMEM((32, DK, DV), BF16),
    a=pltpu.VMEM((32, BLOCK), F32), cum=pltpu.VMEM((32, BLOCK), F32), e=pltpu.VMEM((32, BLOCK), F32),
    fac=pltpu.VMEM((32, BLOCK), F32), run=pltpu.VMEM((2, DK, DV), F32),
    tot_S=pltpu.VMEM((2, DK, DV), F32), tot_f=pltpu.VMEM((2, 1, DV), F32),
    bef_S=pltpu.VMEM((2, DK, DV), F32), bef_f=pltpu.VMEM((2, 1, DV), F32),
    pay_c=pltpu.VMEM((2, PAY, DV), BF16), pay=pltpu.VMEM((2, PAY, DV), BF16), got_c=pltpu.VMEM((1, 2, PAY, DV), BF16),
    got_y=pltpu.VMEM((3, PAY, DV), BF16), got_z=pltpu.VMEM((3, PAY, DV), BF16),
    chip_S=pltpu.VMEM((DK, DV), F32), chip_f=pltpu.VMEM((1, DV), F32), got_e=pltpu.VMEM((DK, DV), F32),
    end_s=DMA, end_r=DMA,
    mix=pltpu.VMEM((512, 2048), BF16), res=pltpu.VMEM((N_TOK, 2048), BF16), out_sem=DMA((4,)), res_sem=DMA,
    in_sem=DMA((5,)), wd_s=DMA((2,)), wd_r=DMA((2,)), wf_s=DMA((2,)), wf_r=DMA((2,)),
    w3_s=DMA, w3_r=DMA,
    pre_s=DMA((7,)), pre_r=DMA((7,)), ret_s=DMA((3,)), ret_r=DMA((3,)),
)


def layer_kernel(
    q, k, v, g, ld, wo, x_ref, gain_ref, rt_ref, wt_ref, wg, wu, wd, sg, su, sd, mix_ref, moe_ref, *scratch
):
    ctx = Ctx()
    s = Names()
    for name, ref in zip(SCRATCH, scratch):
        setattr(s, name, ref)
    greet(ctx)
    a = Names()
    m = Names()
    a.__dict__.update(moe_steps(ctx, x_ref, gain_ref, rt_ref, wt_ref, wg, wu, wd, sg, su, sd, moe_ref, s))
    m.__dict__.update(mixer_steps(ctx, q, k, v, g, ld, wo, mix_ref, s))
    m.fetch()
    a.rows_out()
    a.build(0)
    m.decays()
    m.summary()
    m.publish("ep_2")
    a.shared()
    m.absorb("ep_2")
    m.publish("ep_1")
    a.relay(0)
    m.inside(0, 4)
    a.build(1)
    a.build(3)
    m.spread_d()
    m.absorb("ep_1")
    m.publish("ep_0")
    m.inside(4, 8)
    a.weights()
    a.expert(0)
    a.relay(1)
    a.build(2)
    m.inside(8, 12)
    a.relay(3)
    m.absorb("ep_0")
    m.swap()
    m.inside(12, 16)
    m.settle()
    m.gate_in()
    a.expert(1)
    a.relay(2)
    m.spread_f()
    a.give_back(1)
    m.outer(1)
    m.outer(3)
    m.outer(2)
    a.expert(3)
    a.give_back(3)
    m.outer(0)
    a.expert(2)
    a.give_back(2)
    m.spread_3()
    a.relay_back(1)
    a.relay_back(3)
    a.give_back(0)
    a.fold(1)
    a.relay_back(2)
    a.fold(3)
    m.ready()
    m.project(0, 2)
    a.relay_back(0)
    a.fold(2)
    m.project(2, 4)
    a.fold(0)
    a.finish()
    m.finish()
    m.drain()


def local(
    query_rows, key_rows, value_rows, gate_rows, log_decay, out_proj,
    moe_input, norm_gain, routing, route_weight,
    expert_gate, expert_up, expert_down, shared_gate, shared_up, shared_down,
):
    vm = pl.BlockSpec(memory_space=pltpu.VMEM)
    hbm = pl.BlockSpec(memory_space=pl.ANY)
    return pl.pallas_call(
        layer_kernel,
        name="layer",
        out_shape=(jax.ShapeDtypeStruct((512, 2048), BF16), jax.ShapeDtypeStruct((N_TOK, 2048), BF16)),
        in_specs=[hbm] * 4 + [vm, hbm] + [vm] * 4 + [hbm] * 6,
        out_specs=(hbm, hbm),
        scratch_shapes=list(SCRATCH.values()),
        compiler_params=pltpu.CompilerParams(
            collective_id=0, has_side_effects=True, vmem_limit_bytes=67043328
        ),
    )(
        query_rows, key_rows, value_rows, gate_rows, log_decay, out_proj,
        moe_input, norm_gain.reshape(1, -1), routing.T, route_weight.T,
        expert_gate, expert_up, expert_down, shared_gate, shared_up, shared_down,
    )


def solution(mesh):
    split = Mesh(mesh.devices.reshape(4, 4, 2, mesh.shape["tp"]), ("ep_0", "ep_1", "ep_2", "tp"))
    return jax.shard_map(
        local,
        mesh=split,
        in_specs=(
            P(EP, "tp"),
            P(EP, "tp"),
            P(EP, "tp"),
            P(EP, "tp"),
            P("tp", EP),
            P("tp", None),
            P(EP_TP, None),
            P(),
            P(EP_TP, None),
            P(EP_TP, None),
            P(EP_TP, None, None),
            P(EP_TP, None, None),
            P(EP_TP, None, None),
            P(),
            P(),
            P(),
        ),
        out_specs=(P(EP_TP, None), P(EP_TP, None)),
        check_vma=False,
    )
```
